32 devices in a mesh: sp: 4 (over z), fs: 4 (over y, x), tp: 2 (over core).
Axes of the slice: x: 2, y: 2, z: 4, core: 2. Of those that a mesh axis runs over, the one named last changes fastest.
Arguments:
- tokens: bfloat16 [1024, 2048], P(('sp', 'fs', 'tp')), may hold values from -6 to 6
- norm_gain: float32 [2048], replicated, may hold values from 0.1 to 1.9
- w_query: bfloat16 [2048, 2048], P(None, ('fs', 'tp')), may hold values from -0.9722718 to 0.9722718
- w_key: bfloat16 [2048, 512], P(None, 'fs'), may hold values from -0.77339804 to 0.77339804
- w_value: bfloat16 [2048, 512], P(None, 'fs'), may hold values from -0.125 to 0.125
- w_conv_value: bfloat16 [2048, 1024], P(None, ('fs', 'tp')), may hold values from -0.125 to 0.125
- w_conv_pre: bfloat16 [2048, 1024], P(None, ('fs', 'tp')), may hold values from -0.125 to 0.125
- w_conv_post: bfloat16 [2048, 1024], P(None, ('fs', 'tp')), may hold values from -0.125 to 0.125
- conv_taps: bfloat16 [3, 1024], replicated, may hold values from -3.5 to 3.5
- log_gate_cache: float32 [16, 1024], replicated, may hold values from -65 to 0, as said below
- w_out_conv: bfloat16 [1024, 2048], P(('fs', 'tp')), may hold values from -0.125 to 0.125
- w_out_attn: bfloat16 [2048, 2048], P(('fs', 'tp')), may hold values from -0.375 to 0.375
Outputs:
- mixed: bfloat16 [1024, 2048], P(('sp', 'fs', 'tp'))
The draws below stay inside these ranges and needn't reach their ends.
Inputs may be any that keep to these rules, and one draw needn't show every extreme that they name: `log_gate_cache`: each row is a cumulative sum over positions of log forget gates, none of them positive.
All inputs are finite; a program needn't handle non-finite values.
Results may differ from the reference program's by a relative error of at most 0.014.
The reference program's roundings to bfloat16 on the way count: a program that leaves them out, or rounds other values in their place, can miss the bound.
Values may be sent and summed in bfloat16 or wider, within the bound.
No kernel may reach another device: no remote copies, remote signals or barrier semaphores. Data moves between devices by JAX's collectives and lax.ppermute only.
A program may use at most 64 MiB of HBM per device.

```python
import math
import jax
import jax.numpy as jnp
from jax import lax

D = 2048
QUERY_HEAD_COUNT = 16
KV_HEADS = 4
HEAD_DIM = 128
CHANNELS = 1024
KERNEL = 3
TOK_DEV = 256
SEQUENCE_LENGTH = 1024
N_FS = 4
N_TP = 2


def draw_w_query(key, part):
    entries = jnp.clip(jax.random.normal(jax.random.fold_in(key, 11), (D, QUERY_HEAD_COUNT * HEAD_DIM), jnp.float32), -6.0, 6.0) * (2.5 * D ** (-0.5))
    return entries.astype(jnp.bfloat16)


def draw_w_key(key, part):
    entries = jnp.clip(jax.random.normal(jax.random.fold_in(key, 13), (D, KV_HEADS * HEAD_DIM), jnp.float32), -6.0, 6.0) * D ** (-0.5)
    return entries.astype(jnp.bfloat16)


def draw_log_gate_cache(key, part):
    random_subseeds = jax.random.split(jax.random.fold_in(key, 23), 5)
    head_order = jax.random.permutation(random_subseeds[0], QUERY_HEAD_COUNT)
    fast_count = QUERY_HEAD_COUNT // 2
    fast_heads = head_order < fast_count
    block_count = SEQUENCE_LENGTH // TOK_DEV
    block_rate = jnp.exp(jax.random.uniform(random_subseeds[1], (QUERY_HEAD_COUNT, block_count), jnp.float32, -math.log(2.0), math.log(2.0)))
    jitter = jax.random.uniform(random_subseeds[2], (QUERY_HEAD_COUNT, SEQUENCE_LENGTH), jnp.float32, 0.5, 1.5)
    increment_frequency = jnp.repeat(block_rate, TOK_DEV, axis=1) * jitter
    baseline_frequency = jnp.where(fast_heads[:, None], 1.0 / min(50, TOK_DEV), 0.5 / SEQUENCE_LENGTH)
    spike_position = jax.random.randint(random_subseeds[3], (QUERY_HEAD_COUNT, 3), 0, SEQUENCE_LENGTH)
    spike_length = jax.random.uniform(random_subseeds[4], (QUERY_HEAD_COUNT, 3), jnp.float32, math.log(0.5), math.log(0.8))
    sequence_places = jnp.arange(SEQUENCE_LENGTH, dtype=jnp.int32)
    spike_events = jnp.sum(jnp.where(sequence_places[None, None, :] == spike_position[:, :, None], spike_length[:, :, None], 0.0), axis=1)
    return jnp.cumsum(spike_events - baseline_frequency * increment_frequency, axis=1)


def block_levels(own_key, dims, cuts, least, top_value):
    loudness = 1.0
    for dim, shards_of in cuts:
        heights = jax.random.uniform(jax.random.fold_in(jax.random.fold_in(own_key, 6), dim), (shards_of,), jnp.float32, least / len(cuts), top_value / len(cuts))
        loudness = loudness * jnp.repeat(jnp.exp(heights), dims[dim] // shards_of).reshape((-1,) + (1,) * (len(dims) - 1 - dim))
    return loudness


def gaussian(own_key, extent, scale, limit, pieces=(), kind=jnp.bfloat16):
    result = jax.random.normal(own_key, extent, jnp.float32) * scale
    if len(pieces) > 0:
        result = block_levels(own_key, extent, pieces, -0.22, 0.18) * result
    return jnp.clip(result, min=-limit, max=limit).astype(kind)


def setup_inputs(seed: int = 0) -> dict:
    arg_keys = jax.random.split(jax.random.key(seed), 13)
    return {
        "tokens": gaussian(arg_keys[0], (SEQUENCE_LENGTH, D), 1.0, 6.0, ((0, 32),)),
        "norm_gain": jnp.clip(1.0 + 0.18 * jax.random.normal(arg_keys[1], (D,), jnp.float32), 0.1, 1.9),
        "w_query": draw_w_query(jax.random.fold_in(arg_keys[12], 71), 0),
        "w_key": draw_w_key(jax.random.fold_in(arg_keys[12], 71), 0),
        "w_value": gaussian(arg_keys[4], (D, KV_HEADS * HEAD_DIM), D ** -0.5, 0.125, ((1, 4),)),
        "w_conv_value": gaussian(arg_keys[5], (D, CHANNELS), D ** -0.5, 0.125, ((1, 8),)),
        "w_conv_pre": gaussian(arg_keys[6], (D, CHANNELS), D ** -0.5, 0.125, ((1, 8),)),
        "w_conv_post": gaussian(arg_keys[7], (D, CHANNELS), D ** -0.5, 0.125, ((1, 8),)),
        "conv_taps": gaussian(arg_keys[8], (KERNEL, CHANNELS), KERNEL ** -0.5, 3.5),
        "log_gate_cache": draw_log_gate_cache(jax.random.fold_in(arg_keys[12], 71), 0),
        "w_out_conv": gaussian(arg_keys[10], (CHANNELS, D), (2 * CHANNELS) ** -0.5, 0.125, ((0, 8),)),
        "w_out_attn": gaussian(arg_keys[11], (QUERY_HEAD_COUNT * HEAD_DIM, D), (QUERY_HEAD_COUNT * HEAD_DIM // 8) ** -0.5, 0.375, ((0, 8),)),
    }


epsilon = 1e-06
masked_score = -1e+30

def attend_head(inputs):
    queries, keys, values, head_gates = inputs
    span = 512 if SEQUENCE_LENGTH % 512 == 0 else SEQUENCE_LENGTH
    blocks = SEQUENCE_LENGTH // span
    score_scale = HEAD_DIM ** (-0.5)
    query_blocks = queries.reshape(blocks, span, HEAD_DIM)
    gate_blocks = head_gates.reshape(blocks, span)

    def one_block(block_inputs):
        query_rows, gate_rows, block_index = block_inputs
        row_positions = block_index * span + jnp.arange(span, dtype=jnp.int32)

        def absorb(key_index, carry):
            running_max, running_sum, weighted = carry
            key_start = (key_index * span).astype(jnp.int32)
            key_rows = lax.dynamic_slice_in_dim(keys, key_start, span, 0)
            value_rows = lax.dynamic_slice_in_dim(values, key_start, span, 0)
            gate_keys = lax.dynamic_slice_in_dim(head_gates, key_start, span, 0)
            scores = jnp.dot(query_rows, key_rows.T, preferred_element_type=jnp.float32) * score_scale
            scores = scores + gate_rows[:, None] - gate_keys[None, :]
            key_positions = key_start + jnp.arange(span, dtype=jnp.int32)
            scores = jnp.where(row_positions[:, None] >= key_positions[None, :], scores, masked_score)
            new_max = jnp.maximum(running_max, lax.optimization_barrier(jnp.max(scores, axis=1)))
            rescale = jnp.exp(running_max - new_max)
            weights = jnp.exp(scores - new_max[:, None])
            running_sum = running_sum * rescale + lax.optimization_barrier(jnp.sum(weights, axis=1))
            weighted = weighted * rescale[:, None] + jnp.dot(weights.astype(jnp.bfloat16), value_rows, preferred_element_type=jnp.float32)
            return (new_max, running_sum, weighted)
        initial = (jnp.full((span,), masked_score, jnp.float32), jnp.zeros((span,), jnp.float32), jnp.zeros((span, HEAD_DIM), jnp.float32))
        final = lax.fori_loop(0, block_index + 1, absorb, initial)
        return (final[2] / final[1][:, None]).astype(jnp.bfloat16)
    outputs = lax.map(one_block, (query_blocks, gate_blocks, jnp.arange(blocks, dtype=jnp.int32)))
    return outputs.reshape(SEQUENCE_LENGTH, HEAD_DIM)

def reference(tokens, norm_gain, w_query, w_key, w_value, w_conv_value, w_conv_pre, w_conv_post, conv_taps, log_gate_cache, w_out_conv, w_out_attn):
    float_rows = tokens.astype(jnp.float32)
    normed = (float_rows * lax.rsqrt(lax.optimization_barrier(jnp.mean(float_rows * float_rows, axis=1, keepdims=True)) + epsilon) * norm_gain).astype(jnp.bfloat16)

    def project(weight):
        return jnp.dot(normed, weight, preferred_element_type=jnp.float32).astype(jnp.bfloat16)
    post_gate = project(w_conv_post)
    pre_gate = project(w_conv_pre)
    conv_value = project(w_conv_value)
    queries = project(w_query)
    keys = project(w_key)
    values = project(w_value)
    mixed_in = (pre_gate.astype(jnp.float32) * conv_value.astype(jnp.float32)).astype(jnp.bfloat16)
    padded = jnp.concatenate([jnp.zeros((KERNEL - 1, CHANNELS), jnp.bfloat16), mixed_in], axis=0).astype(jnp.float32)
    tap_weights = conv_taps.astype(jnp.float32)
    conv_sum = tap_weights[0] * padded[0:SEQUENCE_LENGTH]
    for offset in range(1, KERNEL):
        conv_sum = conv_sum + tap_weights[offset] * padded[offset:offset + SEQUENCE_LENGTH]
    conv_out = (post_gate.astype(jnp.float32) * conv_sum).astype(jnp.bfloat16)
    query_heads = queries.reshape(SEQUENCE_LENGTH, QUERY_HEAD_COUNT, HEAD_DIM).transpose(1, 0, 2)
    key_heads = jnp.repeat(keys.reshape(SEQUENCE_LENGTH, KV_HEADS, HEAD_DIM).transpose(1, 0, 2), QUERY_HEAD_COUNT // KV_HEADS, axis=0)
    value_heads = jnp.repeat(values.reshape(SEQUENCE_LENGTH, KV_HEADS, HEAD_DIM).transpose(1, 0, 2), QUERY_HEAD_COUNT // KV_HEADS, axis=0)
    attn_heads = lax.map(attend_head, (query_heads, key_heads, value_heads, log_gate_cache))
    attn_out = attn_heads.transpose(1, 0, 2).reshape(SEQUENCE_LENGTH, QUERY_HEAD_COUNT * HEAD_DIM)
    groups = N_FS * N_TP
    conv_width = CHANNELS // groups
    head_width = QUERY_HEAD_COUNT * HEAD_DIM // groups
    mixed = jnp.zeros((SEQUENCE_LENGTH, D), jnp.float32)
    for group in range(groups):
        partial_sum = jnp.dot(conv_out[:, group * conv_width:(group + 1) * conv_width], w_out_conv[group * conv_width:(group + 1) * conv_width], preferred_element_type=jnp.float32)
        partial_sum = partial_sum + jnp.dot(attn_out[:, group * head_width:(group + 1) * head_width], w_out_attn[group * head_width:(group + 1) * head_width], preferred_element_type=jnp.float32)
        mixed = mixed + lax.optimization_barrier(partial_sum.astype(jnp.bfloat16)).astype(jnp.float32)
    return mixed.astype(jnp.bfloat16)
```

```python
import functools
import math
import jax
import jax.numpy as jnp
from jax import lax
from jax.experimental import pallas as pl
from jax.experimental.pallas import tpu as pltpu
from jax.sharding import PartitionSpec as P

epsilon = 1e-06
masked_score = -1e30
log2e = math.log2(math.e)
f32 = jnp.float32
bf16 = jnp.bfloat16


def kernel_params(mib):
    return pltpu.CompilerParams(vmem_limit_bytes=mib * 1024 * 1024)


def shape_of(rows, cols, dtype=bf16):
    return jax.ShapeDtypeStruct((rows, cols), dtype)


def norm_kernel(tokens_ref, gain_ref, out_ref):
    rows = tokens_ref[...].astype(f32)
    scale = lax.rsqrt(jnp.mean(rows * rows, axis=1, keepdims=True) + epsilon)
    out_ref[...] = (rows * scale * gain_ref[...]).astype(bf16)


def pair_kernel(n_fs, *refs):
    chunks, (w_key, w_value, out_ref, rows_ref) = refs[:n_fs], refs[n_fs:]
    step = chunks[0].shape[0]
    f = lax.axis_index("fs")
    for k in range(n_fs):
        rows_ref[pl.ds(pl.multiple_of((f ^ k) * step, step), step)] = chunks[k][...]
    weight = jnp.concatenate([w_key[...], w_value[...]], axis=1)
    out_ref[...] = jnp.dot(rows_ref[...], weight, preferred_element_type=f32).astype(bf16)


def project_kernel(n_fs, *refs):
    own, other = refs[:n_fs], refs[n_fs : 2 * n_fs]
    w_query, w_post, w_pre, w_conv, w_key, w_value = refs[2 * n_fs : 2 * n_fs + 6]
    q_ref, post_ref, mixed_ref, pair_ref, rows_ref = refs[2 * n_fs + 6 :]
    step = own[0].shape[0]
    lane_rows = n_fs * step
    f = lax.axis_index("fs")
    t = lax.axis_index("tp")
    for k in range(n_fs):
        place = (f ^ k) * step
        rows_ref[pl.ds(pl.multiple_of(t * lane_rows + place, step), step)] = own[k][...]
        rows_ref[pl.ds(pl.multiple_of((1 - t) * lane_rows + place, step), step)] = other[k][...]
    rows = rows_ref[...]
    q_ref[...] = jnp.dot(rows, w_query[...], preferred_element_type=f32).astype(bf16)
    weight = jnp.concatenate([w_pre[...], w_conv[...]], axis=1)
    gated = jnp.dot(rows, weight, preferred_element_type=f32).astype(bf16).astype(f32)
    channels = w_pre.shape[1]
    mixed = (gated[:, :channels] * gated[:, channels:]).astype(bf16)
    post = jnp.dot(rows, w_post[...], preferred_element_type=f32).astype(bf16)
    for lane in range(2):
        for g in range(n_fs):
            source = lane * lane_rows + g * step
            place = g * 2 * step + lane * step
            mixed_ref[place : place + step] = mixed[source : source + step]
            post_ref[place : place + step] = post[source : source + step]
    weight = jnp.concatenate([w_key[...], w_value[...]], axis=1)
    far = rows_ref[pl.ds(pl.multiple_of((1 - t) * lane_rows, lane_rows), lane_rows)]
    pair_ref[...] = jnp.dot(far, weight, preferred_element_type=f32).astype(bf16)


def mixer_kernel(n_sp, n_fs, *refs):
    q_ref, post_ref, mixed_ref, halo_ref, taps_ref, gate_q_ref, gate_k_ref = refs[:7]
    near = refs[7 : 7 + n_sp]
    far = refs[7 + n_sp : 7 + 2 * n_sp]
    w_conv_ref, w_attn_ref, send_ref, keep_ref, extended_ref, conv_ref = refs[7 + 2 * n_sp :]
    z = lax.axis_index("sp")
    t = lax.axis_index("tp")
    block_rows, channels = mixed_ref.shape
    lane_rows = block_rows // 2
    step = lane_rows // n_fs
    head_dim = near[0].shape[1] // 2
    heads = q_ref.shape[1] // head_dim
    edge = halo_ref.shape[0]
    taps = taps_ref.shape[0]
    extended_ref[0:edge] = halo_ref[...].astype(f32)
    extended_ref[edge:] = mixed_ref[...].astype(f32)
    first = edge - (taps - 1)
    conv_sum = taps_ref[0:1] * extended_ref[first : first + block_rows]
    for i in range(1, taps):
        conv_sum = conv_sum + taps_ref[i : i + 1] * extended_ref[first + i : first + i + block_rows]
    conv = (post_ref[...].astype(f32) * conv_sum).astype(bf16)
    for lane in range(2):
        for g in range(n_fs):
            place = lane * lane_rows + g * step
            source = g * 2 * step + lane * step
            conv_ref[place : place + step] = conv[source : source + step]
    scale = head_dim ** (-0.5) * log2e
    row = lax.broadcasted_iota(jnp.int32, (lane_rows, 1), 0)
    col = lax.broadcasted_iota(jnp.int32, (1, block_rows), 1)
    col_lane = jnp.where(col < lane_rows, t, 1 - t)
    inner = jnp.where(col < lane_rows, col, col - lane_rows)
    key_place = (inner // step) * (2 * step) + col_lane * step + inner % step
    for lane, out_ref in ((1 - t, send_ref), (t, keep_ref)):
        base = pl.multiple_of(lane * lane_rows, lane_rows)
        query_place = (row // step) * (2 * step) + lane * step + row % step
        outs = []
        for h in range(heads):
            queries = q_ref[pl.ds(base, lane_rows), h * head_dim : (h + 1) * head_dim]
            gate_q = gate_q_ref[pl.ds(base, lane_rows), h : h + 1] * log2e
            scores = []
            for k in range(n_sp):
                keys = jnp.concatenate(
                    [near[k][:, :head_dim], far[k][:, :head_dim]], axis=0
                )
                zk = jnp.maximum(z - k, 0)
                gate_k = jnp.concatenate(
                    [
                        gate_k_ref[zk, pl.ds(t * heads + h, 1), :],
                        gate_k_ref[zk, pl.ds((1 - t) * heads + h, 1), :],
                    ],
                    axis=1,
                ) * log2e
                gate_k = jnp.where(z >= k, gate_k, -masked_score)
                s = lax.dot_general(
                    queries, keys, (((1,), (1,)), ((), ())), preferred_element_type=f32
                )
                s = s * scale + gate_q - gate_k
                if k == 0:
                    s = jnp.where(query_place >= key_place, s, masked_score)
                scores.append(s)
            top = scores[0]
            for s in scores[1:]:
                top = jnp.maximum(top, s)
            top = jnp.max(top, axis=1, keepdims=True)
            total = 0.0
            weighted = 0.0
            for k in range(n_sp):
                weight = jnp.exp2(scores[k] - top)
                total = total + weight
                values = jnp.concatenate(
                    [near[k][:, head_dim:], far[k][:, head_dim:]], axis=0
                )
                weighted = weighted + jnp.dot(
                    weight.astype(bf16), values, preferred_element_type=f32
                )
            den = jnp.sum(total, axis=1, keepdims=True)
            outs.append((weighted / den).astype(bf16))
        attn = jnp.concatenate(outs, axis=1)
        out = jnp.dot(conv_ref[pl.ds(base, lane_rows)], w_conv_ref[...], preferred_element_type=f32)
        out = out + jnp.dot(attn, w_attn_ref[...], preferred_element_type=f32)
        out_ref[...] = out.astype(bf16)


def pair_sum_kernel(n_fs, keep_ref, got_ref, *outs):
    f = lax.axis_index("fs")
    step = outs[0].shape[0]
    for k in range(n_fs):
        rows = pl.ds(pl.multiple_of((f ^ k) * step, step), step)
        total = keep_ref[rows].astype(f32) + got_ref[rows].astype(f32)
        outs[k][...] = total.astype(outs[k].dtype)


def final_kernel(*refs):
    total = refs[0][...].astype(f32)
    for ref in refs[1:-1]:
        total = total + ref[...].astype(f32)
    refs[-1][...] = total.astype(bf16)


def layer(
    tokens,
    norm_gain,
    w_query,
    w_key,
    w_value,
    w_conv_value,
    w_conv_pre,
    w_conv_post,
    conv_taps,
    log_gate_cache,
    w_out_conv,
    w_out_attn,
):
    n_sp, n_fs, n_tp = lax.axis_size("sp"), lax.axis_size("fs"), lax.axis_size("tp")
    step, width = tokens.shape
    lane_rows = n_fs * step
    block_rows = n_tp * lane_rows
    channels = w_conv_post.shape[1]
    head_dim = w_key.shape[1]
    heads = w_query.shape[1] // head_dim
    group = lax.axis_index(("fs", "tp"))
    z = lax.axis_index("sp")

    def swapped(x):
        return lax.ppermute(x, "tp", [(0, 1), (1, 0)])

    def crossed(x, k):
        return lax.ppermute(x, "fs", [(i, i ^ k) for i in range(n_fs)])

    def raised(x, k):
        return lax.ppermute(x, "sp", [(i, i + k) for i in range(n_sp - k)])

    head_gates = lax.dynamic_slice_in_dim(log_gate_cache, group * heads, heads, 0)
    head_gates = head_gates.reshape(heads, n_sp, n_fs, n_tp, step).transpose(1, 3, 0, 2, 4)
    gate_k = head_gates.reshape(n_sp, n_tp * heads, lane_rows)
    gate_q = lax.dynamic_index_in_dim(head_gates, z, 0, False)
    gate_q = gate_q.transpose(0, 2, 3, 1).reshape(block_rows, heads)
    taps = lax.dynamic_slice_in_dim(conv_taps, group * channels, channels, 1).astype(f32)

    normed = pl.pallas_call(
        norm_kernel, out_shape=shape_of(step, width), compiler_params=kernel_params(4)
    )(tokens, norm_gain.reshape(1, width))
    own = [normed] + [crossed(normed, k) for k in range(1, n_fs)]
    other = [swapped(x) for x in own]
    near = [
        pl.pallas_call(
            functools.partial(pair_kernel, n_fs),
            out_shape=shape_of(lane_rows, 2 * head_dim),
            scratch_shapes=[pltpu.VMEM((lane_rows, width), bf16)],
            compiler_params=kernel_params(8),
        )(*own, w_key, w_value)
    ]
    near += [raised(near[0], k) for k in range(1, n_sp)]
    queries, post, mixed, far_own = pl.pallas_call(
        functools.partial(project_kernel, n_fs),
        out_shape=(
            shape_of(block_rows, heads * head_dim),
            shape_of(block_rows, channels),
            shape_of(block_rows, channels),
            shape_of(lane_rows, 2 * head_dim),
        ),
        scratch_shapes=[pltpu.VMEM((block_rows, width), bf16)],
        compiler_params=kernel_params(16),
    )(*own, *other, w_query, w_conv_post, w_conv_pre, w_conv_value, w_key, w_value)
    halo = raised(mixed[block_rows - 16 :], 1)
    far = [far_own] + [swapped(x) for x in near[1:]]
    send, keep = pl.pallas_call(
        functools.partial(mixer_kernel, n_sp, n_fs),
        out_shape=(shape_of(lane_rows, width), shape_of(lane_rows, width)),
        scratch_shapes=[
            pltpu.VMEM((block_rows + 16, channels), f32),
            pltpu.VMEM((block_rows, channels), bf16),
        ],
        compiler_params=kernel_params(24),
    )(queries, post, mixed, halo, taps, gate_q, gate_k, *near, *far, w_out_conv, w_out_attn)
    got = swapped(send)
    sums = pl.pallas_call(
        functools.partial(pair_sum_kernel, n_fs),
        out_shape=tuple(shape_of(step, width, f32 if k == 0 else bf16) for k in range(n_fs)),
        compiler_params=kernel_params(8),
    )(keep, got)
    parts = [sums[0]] + [crossed(sums[k], k) for k in range(1, n_fs)]
    return pl.pallas_call(
        final_kernel, out_shape=shape_of(step, width), compiler_params=kernel_params(4)
    )(*parts)


def passed_along(block, axis, distance):
    devices = range(lax.axis_size(axis))
    route = [(i - distance, i) for i in devices if i - distance in devices]
    return lax.ppermute(block, axis, route)


def shards(
    tokens,
    norm_gain,
    w_query,
    w_key,
    w_value,
    w_conv_value,
    w_conv_pre,
    w_conv_post,
    conv_taps,
    log_gate_cache,
    w_out_conv,
    w_out_attn,
):
    float_rows = tokens.astype(jnp.float32)
    scaled = float_rows * lax.rsqrt(
        jnp.mean(float_rows * float_rows, axis=1, keepdims=True) + epsilon
    )
    normed_own = (scaled * norm_gain).astype(jnp.bfloat16)
    normed = lax.all_gather(normed_own, ("fs", "tp"), axis=0, tiled=True)
    block_rows = normed.shape[0]
    channels = w_conv_post.shape[1]
    head_dim = w_key.shape[1]
    local_heads = w_query.shape[1] // head_dim
    group = lax.axis_index(("fs", "tp"))
    local_weight = jnp.concatenate([w_conv_post, w_conv_pre, w_conv_value, w_query], axis=1)
    projected = jnp.dot(normed, local_weight, preferred_element_type=jnp.float32).astype(
        jnp.bfloat16
    )
    post_gate = projected[:, :channels]
    pre_gate = projected[:, channels : 2 * channels]
    conv_value = projected[:, 2 * channels : 3 * channels]
    queries = projected[:, 3 * channels :].reshape(block_rows, local_heads, head_dim)
    mixed_in = (pre_gate.astype(jnp.float32) * conv_value.astype(jnp.float32)).astype(jnp.bfloat16)
    kernel = conv_taps.shape[0]
    carried = passed_along(mixed_in[block_rows - (kernel - 1) :], "sp", 1)
    extended = jnp.concatenate([carried, mixed_in], axis=0).astype(jnp.float32)
    tap_weights = lax.dynamic_slice_in_dim(conv_taps, group * channels, channels, 1).astype(
        jnp.float32
    )
    conv_sum = tap_weights[0] * extended[0:block_rows]
    for offset in range(1, kernel):
        conv_sum = conv_sum + tap_weights[offset] * extended[offset : offset + block_rows]
    conv_out = (post_gate.astype(jnp.float32) * conv_sum).astype(jnp.bfloat16)
    core_index = lax.axis_index("tp")
    half_rows = block_rows // 2
    own_rows = lax.dynamic_slice_in_dim(normed, core_index * half_rows, half_rows, 0)
    pair_weight = jnp.concatenate([w_key, w_value], axis=1)
    pair_rows = jnp.dot(own_rows, pair_weight, preferred_element_type=jnp.float32).astype(
        jnp.bfloat16
    )
    key_half = pair_rows[:, :head_dim]
    value_half = pair_rows[:, head_dim:]
    head_gates = lax.dynamic_slice_in_dim(log_gate_cache, group * local_heads, local_heads, 0)
    anchor = lax.axis_index("sp") * block_rows
    gate_query = lax.dynamic_slice_in_dim(head_gates, anchor, block_rows, 1).T
    sequence_places = anchor + lax.iota(jnp.int32, block_rows)
    score_scale = head_dim ** (-0.5)

    def absorb(carried_state, key_block, value_block, sub_start):
        running_max, running_sum, weighted = carried_state
        sub_width = key_block.shape[0]
        scores = (
            jnp.einsum("qhd,kd->qhk", queries, key_block, preferred_element_type=jnp.float32)
            * score_scale
        )
        gate_keys = lax.dynamic_slice_in_dim(head_gates, sub_start, sub_width, 1)
        scores = scores + gate_query[:, :, None] - gate_keys[None, :, :]
        key_positions = sub_start + lax.iota(jnp.int32, sub_width)
        scores = jnp.where(
            sequence_places[:, None, None] >= key_positions[None, None, :], scores, masked_score
        )
        new_max = jnp.maximum(running_max, jnp.max(scores, axis=2))
        rescale = jnp.exp(running_max - new_max)
        weights = jnp.exp(scores - new_max[:, :, None])
        running_sum = running_sum * rescale + jnp.sum(weights, axis=2)
        weighted = weighted * rescale[:, :, None] + jnp.einsum(
            "qhk,kd->qhd",
            weights.astype(jnp.bfloat16),
            value_block,
            preferred_element_type=jnp.float32,
        )
        return (new_max, running_sum, weighted)

    initial = (
        jnp.full((block_rows, local_heads), masked_score, jnp.float32),
        jnp.zeros((block_rows, local_heads), jnp.float32),
        jnp.zeros((block_rows, local_heads, head_dim), jnp.float32),
    )
    key_piece = lax.all_gather(key_half, ("sp", "tp"), axis=0, tiled=True)
    value_piece = lax.all_gather(value_half, ("sp", "tp"), axis=0, tiled=True)
    key_count = key_piece.shape[0]
    sub_width = 512

    def sweep_keys(current):

        def absorb_step(running, step_index):
            sub_start = step_index * sub_width
            key_block = lax.dynamic_slice_in_dim(key_piece, sub_start, sub_width, 0)
            value_block = lax.dynamic_slice_in_dim(value_piece, sub_start, sub_width, 0)
            return (absorb(running, key_block, value_block, sub_start), None)

        result, unused = lax.scan(
            absorb_step, current, jnp.arange(key_count // sub_width, dtype=jnp.int32)
        )
        return result

    def keep_state(current):
        return current

    running_max, running_sum, weighted = lax.cond(
        jnp.int32(0) <= anchor + block_rows - 1, sweep_keys, keep_state, initial
    )
    attn_out = (
        (weighted / running_sum[:, :, None])
        .astype(jnp.bfloat16)
        .reshape(block_rows, local_heads * head_dim)
    )
    return lax.psum_scatter(
        (
            jnp.dot(conv_out, w_out_conv, preferred_element_type=jnp.float32)
            + jnp.dot(attn_out, w_out_attn, preferred_element_type=jnp.float32)
        ).astype(jnp.bfloat16),
        ("fs", "tp"),
        scatter_dimension=0,
        tiled=True,
    )


def solution(mesh):
    few = mesh.shape["sp"] <= 8
    placed = (
        P(("sp", "fs", "tp"), None),
        P(),
        P(None, ("fs", "tp")),
        P(None, "fs"),
        P(None, "fs"),
        P(None, ("fs", "tp")),
        P(None, ("fs", "tp")),
        P(None, ("fs", "tp")),
        P(),
        P(),
        P(("fs", "tp"), None),
        P(("fs", "tp"), None),
    )
    return jax.shard_map(
        layer if few else shards, mesh=mesh, in_specs=placed, out_specs=P(("sp", "fs", "tp"), None), check_vma=False
    )
```

```python
import functools
import math
import jax
import jax.numpy as jnp
from jax import lax
from jax.experimental import pallas as pl
from jax.experimental.pallas import tpu as pltpu
from jax.sharding import PartitionSpec as P

epsilon = 1e-06
masked_score = -1e30
log2e = math.log2(math.e)
f32 = jnp.float32
bf16 = jnp.bfloat16
EDGE = 16
RING = True
NORM_WORK = 20000000000
MASK_WORK = 2000000000
SMALL_WORK = 2000000000


def kernel_params(mib):
    return pltpu.CompilerParams(vmem_limit_bytes=mib * 1024 * 1024)


def shape_of(rows, cols, dtype=bf16):
    return jax.ShapeDtypeStruct((rows, cols), dtype)


def mask_kernel(out_ref):
    query_place = lax.broadcasted_iota(jnp.int32, out_ref.shape, 0)
    key_place = lax.broadcasted_iota(jnp.int32, out_ref.shape, 1)
    out_ref[...] = jnp.where(query_place >= key_place, 0.0, masked_score)


def norm_kernel(tokens_ref, gain_ref, out_ref):
    rows = tokens_ref[...].astype(f32)
    scale = lax.rsqrt(jnp.mean(rows * rows, axis=1, keepdims=True) + epsilon)
    out_ref[...] = (rows * scale * gain_ref[...]).astype(bf16)


def pair_kernel(n_fs, *refs):
    chunks, (w_key, w_value, out_ref, rows_ref) = refs[:n_fs], refs[n_fs:]
    step = chunks[0].shape[0]
    f = lax.axis_index("fs")
    for k in range(n_fs):
        rows_ref[pl.ds(pl.multiple_of((f ^ k) * step, step), step)] = chunks[k][...]
    weight = jnp.concatenate([w_key[...], w_value[...]], axis=1)
    out_ref[...] = jnp.dot(rows_ref[...], weight, preferred_element_type=f32).astype(bf16)


def join_kernel(n_fs, near_ref, far_ref, out_ref):
    step = near_ref.shape[0] // n_fs
    t = lax.axis_index("tp")
    for lane, piece in ((t, near_ref), (1 - t, far_ref)):
        for g in range(n_fs):
            place = pl.ds(pl.multiple_of(g * 2 * step + lane * step, step), step)
            out_ref[place] = piece[g * step : (g + 1) * step]


def project_kernel(n_fs, *refs):
    own, other = refs[:n_fs], refs[n_fs : 2 * n_fs]
    w_query, w_post, w_pre, w_conv, near_ref = refs[2 * n_fs : 2 * n_fs + 5]
    q_ref, post_ref, mixed_ref, rise_ref, rows_ref = refs[2 * n_fs + 5 :]
    step = own[0].shape[0]
    f = lax.axis_index("fs")
    t = lax.axis_index("tp")
    for k in range(n_fs):
        place = (f ^ k) * (2 * step)
        rows_ref[pl.ds(pl.multiple_of(place + t * step, step), step)] = own[k][...]
        rows_ref[pl.ds(pl.multiple_of(place + (1 - t) * step, step), step)] = other[k][...]
    rows = rows_ref[...]
    weight = jnp.concatenate([w_pre[...], w_conv[...]], axis=1)
    gated = jnp.dot(rows, weight, preferred_element_type=f32).astype(bf16).astype(f32)
    channels = w_pre.shape[1]
    mixed = (gated[:, :channels] * gated[:, channels:]).astype(bf16)
    mixed_ref[...] = mixed
    lane_rows = near_ref.shape[0]
    rise_ref[:lane_rows] = near_ref[...]
    rise_ref[lane_rows:, :channels] = mixed[mixed.shape[0] - EDGE :]
    rise_ref[lane_rows:, channels:] = mixed[mixed.shape[0] - EDGE :]
    q_ref[...] = jnp.dot(rows, w_query[...], preferred_element_type=f32).astype(bf16)
    post_ref[...] = jnp.dot(rows, w_post[...], preferred_element_type=f32).astype(bf16)


def conv_kernel(post_ref, mixed_ref, risen_ref, taps_ref, out_ref, extended_ref):
    block_rows, channels = mixed_ref.shape
    group = lax.axis_index("fs") * lax.axis_size("tp") + lax.axis_index("tp")
    lanes = pl.ds(pl.multiple_of(group * channels, channels), channels)
    edge = EDGE
    taps = taps_ref.shape[0]
    halo = risen_ref[risen_ref.shape[0] - edge :, :channels].astype(f32)
    extended_ref[0:edge] = jnp.where(lax.axis_index("sp") > 0, halo, 0.0)
    extended_ref[edge:] = mixed_ref[...].astype(f32)
    tap_rows = taps_ref[:, lanes].astype(f32)
    first = edge - (taps - 1)
    conv_sum = tap_rows[0:1] * extended_ref[first : first + block_rows]
    for i in range(1, taps):
        conv_sum = conv_sum + tap_rows[i : i + 1] * extended_ref[first + i : first + i + block_rows]
    out_ref[...] = (post_ref[...].astype(f32) * conv_sum).astype(bf16)


def mixer_kernel(n_fs, parts, *refs):
    q_ref, conv_in_ref, gates_ref, mask_ref, block_ref = refs[:5]
    near_ref, far_ref, high_ref, low_ref = refs[5:9]
    w_conv_ref, w_attn_ref, send_ref, keep_ref = refs[9:13]
    key_ref, value_ref, gate_col_ref, tile_ref, conv_ref, sum_ref = refs[13:]
    z = lax.axis_index("sp")
    f = lax.axis_index("fs")
    t = lax.axis_index("tp")
    block_rows = conv_in_ref.shape[0]
    step = block_rows // (2 * n_fs)
    head_dim = block_ref.shape[1] // 2
    heads = q_ref.shape[1] // head_dim
    group = f * 2 + t
    count = len(parts)
    rows = count * 2 * step
    for lane, piece in ((t, near_ref), (1 - t, far_ref)):
        for g in range(n_fs):
            place = pl.ds(pl.multiple_of(g * 2 * step + lane * step, step), step)
            key_ref[place] = piece[g * step : (g + 1) * step, :head_dim]
            value_ref[place] = piece[g * step : (g + 1) * step, head_dim:]
    key_blocks = [block_ref[:, :head_dim], key_ref[...], high_ref[:, :head_dim], low_ref[:, :head_dim]]
    value_blocks = [
        block_ref[:, head_dim:],
        value_ref[...],
        high_ref[:, head_dim:],
        low_ref[:, head_dim:],
    ]
    origins = [z, z - 1, z - 2 - t, z - 3 + t]
    n_blocks = len(origins)

    def gate_row(h, origin):
        place = pl.multiple_of(jnp.maximum(origin, 0) * block_rows, block_rows)
        return gates_ref[pl.ds(group * heads + h, 1), pl.ds(place, block_rows)] * log2e

    for h in range(heads):
        column = jnp.broadcast_to(gate_row(h, z), (8, block_rows)).T
        gate_col_ref[h] = column
    scale = head_dim ** (-0.5) * log2e
    bases = [pl.multiple_of((f ^ part) * (2 * step), 2 * step) for part in parts]
    for h in range(heads):
        for i, base in enumerate(bases):
            place = (h * count + i) * 2 * step
            tile_ref[place : place + 2 * step] = q_ref[
                pl.ds(base, 2 * step), h * head_dim : (h + 1) * head_dim
            ]
    mask = jnp.concatenate([mask_ref[pl.ds(base, 2 * step)] for base in bases], axis=0)
    outs = []
    for h in range(heads):
        queries = tile_ref[h * rows : (h + 1) * rows]
        gate_q = jnp.concatenate(
            [gate_col_ref[h, pl.ds(base, 2 * step), 0:1] for base in bases], axis=0
        )
        scores = []
        for k in range(n_blocks):
            s = lax.dot_general(
                queries,
                key_blocks[k],
                (((1,), (1,)), ((), ())),
                preferred_element_type=f32,
            )
            gate_k = jnp.where(origins[k] >= 0, gate_row(h, origins[k]), -masked_score)
            s = s * scale + gate_q - gate_k
            if k == 0:
                s = s + mask
            scores.append(s)
        top = scores[0]
        for s in scores[1:]:
            top = jnp.maximum(top, s)
        top = jnp.max(top, axis=1, keepdims=True)
        total = 0.0
        weighted = 0.0
        for k in range(n_blocks):
            weight = jnp.exp2(scores[k] - top)
            total = total + weight
            weighted = weighted + jnp.dot(
                weight.astype(bf16),
                value_blocks[k],
                preferred_element_type=f32,
            )
        den = jnp.sum(total, axis=1, keepdims=True)
        outs.append((weighted / den).astype(bf16))
    attn = jnp.concatenate(outs, axis=1)
    for i, base in enumerate(bases):
        conv_ref[i * 2 * step : (i + 1) * 2 * step] = conv_in_ref[pl.ds(base, 2 * step)]
    out = jnp.dot(conv_ref[...], w_conv_ref[...], preferred_element_type=f32)
    out = out + jnp.dot(attn, w_attn_ref[...], preferred_element_type=f32)
    sum_ref[...] = out.astype(bf16)
    for i in range(count):
        place = i * 2 * step
        mine = pl.ds(pl.multiple_of(place + t * step, step), step)
        theirs = pl.ds(pl.multiple_of(place + (1 - t) * step, step), step)
        keep_ref[i * step : (i + 1) * step] = sum_ref[mine]
        send_ref[i * step : (i + 1) * step] = sum_ref[theirs]


def pair_sum_kernel(keep_ref, got_ref, *outs):
    step = outs[0].shape[0]
    for i, out in enumerate(outs):
        rows = slice(i * step, (i + 1) * step)
        total = keep_ref[rows].astype(f32) + got_ref[rows].astype(f32)
        out[...] = total.astype(out.dtype)


def final_kernel(*refs):
    total = refs[0][...].astype(f32)
    for ref in refs[1:-1]:
        total = total + ref[...].astype(f32)
    refs[-1][...] = total.astype(bf16)


def layer(
    tokens,
    norm_gain,
    w_query,
    w_key,
    w_value,
    w_conv_value,
    w_conv_pre,
    w_conv_post,
    conv_taps,
    log_gate_cache,
    w_out_conv,
    w_out_attn,
):
    n_sp, n_fs, n_tp = lax.axis_size("sp"), lax.axis_size("fs"), lax.axis_size("tp")
    step, width = tokens.shape
    lane_rows = n_fs * step
    block_rows = n_tp * lane_rows
    channels = w_conv_post.shape[1]
    head_dim = w_key.shape[1]
    heads = w_query.shape[1] // head_dim
    partition = (tuple(range(n_fs - 1, -1, -1)),)

    def swapped(x):
        return lax.ppermute(x, "tp", [(0, 1), (1, 0)])

    def crossed(x, k):
        return lax.ppermute(x, "fs", [(i, i ^ k) for i in range(n_fs)])

    def raised(x, shifts):
        route = [
            (i * n_tp + t, (i + shift) % n_sp * n_tp + t)
            for t, shift in enumerate(shifts)
            for i in range(n_sp)
            if i + shift < n_sp or RING
        ]
        return lax.ppermute(x, ("sp", "tp"), route)

    def call(kernel, out_shape, scratch, mib, *operands, in_specs=None, work=0):
        extra = {} if in_specs is None else {"in_specs": in_specs}
        if work:
            extra["cost_estimate"] = pl.CostEstimate(
                flops=work, transcendentals=0, bytes_accessed=0
            )
        return pl.pallas_call(
            kernel,
            out_shape=out_shape,
            scratch_shapes=scratch,
            compiler_params=kernel_params(mib),
            **extra,
        )(*operands)

    mask = call(mask_kernel, shape_of(block_rows, block_rows, f32), [], 4, work=MASK_WORK)
    normed = call(
        norm_kernel,
        shape_of(step, width),
        [],
        4,
        tokens,
        norm_gain.reshape(1, width),
        work=NORM_WORK,
    )
    w_post, w_pre, w_conv = w_conv_post, w_conv_pre, w_conv_value
    gates, taps = log_gate_cache, conv_taps
    own = [normed] + [crossed(normed, k) for k in range(1, n_fs)]
    other = [swapped(x) for x in own]
    pair = call(
        functools.partial(pair_kernel, n_fs),
        shape_of(lane_rows, 2 * head_dim),
        [pltpu.VMEM((lane_rows, width), bf16)],
        8,
        *own,
        w_key,
        w_value,
        work=SMALL_WORK,
    )
    block = call(
        functools.partial(join_kernel, n_fs),
        shape_of(block_rows, 2 * head_dim),
        [],
        4,
        pair,
        swapped(pair),
    )
    high = raised(block, (2, 3))
    queries, post, mixed, rise = call(
        functools.partial(project_kernel, n_fs),
        (
            shape_of(block_rows, heads * head_dim),
            shape_of(block_rows, channels),
            shape_of(block_rows, channels),
            shape_of(lane_rows + EDGE, 2 * head_dim),
        ),
        [pltpu.VMEM((block_rows, width), bf16)],
        16,
        *own,
        *other,
        w_query,
        w_post,
        w_pre,
        w_conv,
        pair,
        work=SMALL_WORK,
    )
    near = raised(rise, (1, 1))
    far = swapped(near)
    low = swapped(high)
    conv_out = call(
        conv_kernel,
        shape_of(block_rows, channels),
        [pltpu.VMEM((block_rows + EDGE, channels), f32)],
        4,
        post,
        mixed,
        near,
        taps,
        work=SMALL_WORK,
    )
    sums = {}
    for parts in partition:
        count = len(parts)
        send, keep = call(
            functools.partial(mixer_kernel, n_fs, parts),
            (shape_of(count * step, width), shape_of(count * step, width)),
            [
                pltpu.VMEM((block_rows, head_dim), bf16),
                pltpu.VMEM((block_rows, head_dim), bf16),
                pltpu.VMEM((heads, block_rows, 8), f32),
                pltpu.VMEM((heads * count * 2 * step, head_dim), bf16),
                pltpu.VMEM((count * 2 * step, channels), bf16),
                pltpu.VMEM((count * 2 * step, width), bf16),
            ],
            16,
            queries,
            conv_out,
            gates,
            mask,
            block,
            near,
            far,
            high,
            low,
            w_out_conv,
            w_out_attn,
        )
        got = swapped(send)
        pieces = call(
            pair_sum_kernel,
            tuple(shape_of(step, width, f32 if k == 0 else bf16) for k in parts),
            [],
            8,
            keep,
            got,
        )
        for k, piece in zip(parts, pieces):
            sums[k] = crossed(piece, k) if k else piece
    return call(final_kernel, shape_of(step, width), [], 4, *[sums[k] for k in range(n_fs)])


def passed_along(block, axis, distance):
    devices = range(lax.axis_size(axis))
    route = [(i - distance, i) for i in devices if i - distance in devices]
    return lax.ppermute(block, axis, route)


def shards(
    tokens,
    norm_gain,
    w_query,
    w_key,
    w_value,
    w_conv_value,
    w_conv_pre,
    w_conv_post,
    conv_taps,
    log_gate_cache,
    w_out_conv,
    w_out_attn,
):
    float_rows = tokens.astype(jnp.float32)
    scaled = float_rows * lax.rsqrt(
        jnp.mean(float_rows * float_rows, axis=1, keepdims=True) + epsilon
    )
    normed_own = (scaled * norm_gain).astype(jnp.bfloat16)
    normed = lax.all_gather(normed_own, ("fs", "tp"), axis=0, tiled=True)
    block_rows = normed.shape[0]
    channels = w_conv_post.shape[1]
    head_dim = w_key.shape[1]
    local_heads = w_query.shape[1] // head_dim
    group = lax.axis_index(("fs", "tp"))
    local_weight = jnp.concatenate([w_conv_post, w_conv_pre, w_conv_value, w_query], axis=1)
    projected = jnp.dot(normed, local_weight, preferred_element_type=jnp.float32).astype(
        jnp.bfloat16
    )
    post_gate = projected[:, :channels]
    pre_gate = projected[:, channels : 2 * channels]
    conv_value = projected[:, 2 * channels : 3 * channels]
    queries = projected[:, 3 * channels :].reshape(block_rows, local_heads, head_dim)
    mixed_in = (pre_gate.astype(jnp.float32) * conv_value.astype(jnp.float32)).astype(jnp.bfloat16)
    kernel = conv_taps.shape[0]
    carried = passed_along(mixed_in[block_rows - (kernel - 1) :], "sp", 1)
    extended = jnp.concatenate([carried, mixed_in], axis=0).astype(jnp.float32)
    tap_weights = lax.dynamic_slice_in_dim(conv_taps, group * channels, channels, 1).astype(
        jnp.float32
    )
    conv_sum = tap_weights[0] * extended[0:block_rows]
    for offset in range(1, kernel):
        conv_sum = conv_sum + tap_weights[offset] * extended[offset : offset + block_rows]
    conv_out = (post_gate.astype(jnp.float32) * conv_sum).astype(jnp.bfloat16)
    core_index = lax.axis_index("tp")
    half_rows = block_rows // 2
    own_rows = lax.dynamic_slice_in_dim(normed, core_index * half_rows, half_rows, 0)
    pair_weight = jnp.concatenate([w_key, w_value], axis=1)
    pair_rows = jnp.dot(own_rows, pair_weight, preferred_element_type=jnp.float32).astype(
        jnp.bfloat16
    )
    key_half = pair_rows[:, :head_dim]
    value_half = pair_rows[:, head_dim:]
    head_gates = lax.dynamic_slice_in_dim(log_gate_cache, group * local_heads, local_heads, 0)
    anchor = lax.axis_index("sp") * block_rows
    gate_query = lax.dynamic_slice_in_dim(head_gates, anchor, block_rows, 1).T
    sequence_places = anchor + lax.iota(jnp.int32, block_rows)
    score_scale = head_dim ** (-0.5)

    def absorb(carried_state, key_block, value_block, sub_start):
        running_max, running_sum, weighted = carried_state
        sub_width = key_block.shape[0]
        scores = (
            jnp.einsum("qhd,kd->qhk", queries, key_block, preferred_element_type=jnp.float32)
            * score_scale
        )
        gate_keys = lax.dynamic_slice_in_dim(head_gates, sub_start, sub_width, 1)
        scores = scores + gate_query[:, :, None] - gate_keys[None, :, :]
        key_positions = sub_start + lax.iota(jnp.int32, sub_width)
        scores = jnp.where(
            sequence_places[:, None, None] >= key_positions[None, None, :], scores, masked_score
        )
        new_max = jnp.maximum(running_max, jnp.max(scores, axis=2))
        rescale = jnp.exp(running_max - new_max)
        weights = jnp.exp(scores - new_max[:, :, None])
        running_sum = running_sum * rescale + jnp.sum(weights, axis=2)
        weighted = weighted * rescale[:, :, None] + jnp.einsum(
            "qhk,kd->qhd",
            weights.astype(jnp.bfloat16),
            value_block,
            preferred_element_type=jnp.float32,
        )
        return (new_max, running_sum, weighted)

    initial = (
        jnp.full((block_rows, local_heads), masked_score, jnp.float32),
        jnp.zeros((block_rows, local_heads), jnp.float32),
        jnp.zeros((block_rows, local_heads, head_dim), jnp.float32),
    )
    key_piece = lax.all_gather(key_half, ("sp", "tp"), axis=0, tiled=True)
    value_piece = lax.all_gather(value_half, ("sp", "tp"), axis=0, tiled=True)
    key_count = key_piece.shape[0]
    sub_width = 512

    def sweep_keys(current):

        def absorb_step(running, step_index):
            sub_start = step_index * sub_width
            key_block = lax.dynamic_slice_in_dim(key_piece, sub_start, sub_width, 0)
            value_block = lax.dynamic_slice_in_dim(value_piece, sub_start, sub_width, 0)
            return (absorb(running, key_block, value_block, sub_start), None)

        result, _ = lax.scan(
            absorb_step, current, jnp.arange(key_count // sub_width, dtype=jnp.int32)
        )
        return result

    def keep_state(current):
        return current

    _, running_sum, weighted = lax.cond(
        jnp.int32(0) <= anchor + block_rows - 1, sweep_keys, keep_state, initial
    )
    attn_out = (
        (weighted / running_sum[:, :, None])
        .astype(jnp.bfloat16)
        .reshape(block_rows, local_heads * head_dim)
    )
    return lax.psum_scatter(
        (
            jnp.dot(conv_out, w_out_conv, preferred_element_type=jnp.float32)
            + jnp.dot(attn_out, w_out_attn, preferred_element_type=jnp.float32)
        ).astype(jnp.bfloat16),
        ("fs", "tp"),
        scatter_dimension=0,
        tiled=True,
    )


def solution(mesh):
    few = mesh.shape["sp"] == 4
    placed = (
        P(("sp", "fs", "tp"), None),
        P(),
        P(None, ("fs", "tp")),
        P(None, "fs"),
        P(None, "fs"),
        P(None, ("fs", "tp")),
        P(None, ("fs", "tp")),
        P(None, ("fs", "tp")),
        P(),
        P(),
        P(("fs", "tp"), None),
        P(("fs", "tp"), None),
    )
    return jax.shard_map(
        layer if few else shards,
        mesh=mesh,
        in_specs=placed,
        out_specs=P(("sp", "fs", "tp"), None),
        check_vma=False,
    )
```

```python
import functools
import math
import jax
import jax.numpy as jnp
from jax import lax
from jax.experimental import pallas as pl
from jax.experimental.pallas import tpu as pltpu
from jax.sharding import PartitionSpec as P

epsilon = 1e-06
masked_score = -1e30
log2e = math.log2(math.e)
f32 = jnp.float32
bf16 = jnp.bfloat16
EDGE = 16
RING = True
NORM_WORK = 20000000000
MASK_WORK = 2000000000
SMALL_WORK = 2000000000


def kernel_params(mib):
    return pltpu.CompilerParams(vmem_limit_bytes=mib * 1024 * 1024)


def shape_of(rows, cols, dtype=bf16):
    return jax.ShapeDtypeStruct((rows, cols), dtype)


def mask_kernel(out_ref):
    query_place = lax.broadcasted_iota(jnp.int32, out_ref.shape, 0)
    key_place = lax.broadcasted_iota(jnp.int32, out_ref.shape, 1)
    out_ref[...] = jnp.where(query_place >= key_place, 0.0, masked_score)


def norm_kernel(tokens_ref, gain_ref, out_ref):
    rows = tokens_ref[...].astype(f32)
    scale = lax.rsqrt(jnp.mean(rows * rows, axis=1, keepdims=True) + epsilon)
    out_ref[...] = (rows * scale * gain_ref[...]).astype(bf16)


def pair_kernel(n_fs, *refs):
    chunks, (w_key, w_value, out_ref, rows_ref) = refs[:n_fs], refs[n_fs:]
    step = chunks[0].shape[0]
    f = lax.axis_index("fs")
    for k in range(n_fs):
        rows_ref[pl.ds(pl.multiple_of((f ^ k) * step, step), step)] = chunks[k][...]
    weight = jnp.concatenate([w_key[...], w_value[...]], axis=1)
    out_ref[...] = jnp.dot(rows_ref[...], weight, preferred_element_type=f32).astype(bf16)


def place_pairs(pieces, key_ref, value_ref):
    head_dim = key_ref.shape[1]
    t = lax.axis_index("tp")
    n_fs = lax.axis_size("fs")
    step = key_ref.shape[0] // (2 * n_fs * len(pieces))
    for k, (near, far) in enumerate(pieces):
        for lane, piece in ((t, near), (1 - t, far)):
            for g in range(n_fs):
                place = (k * n_fs + g) * 2 * step + lane * step
                place = pl.ds(pl.multiple_of(place, step), step)
                key_ref[place] = piece[g * step : (g + 1) * step, :head_dim]
                value_ref[place] = piece[g * step : (g + 1) * step, head_dim:]


def gate_row(gates_ref, h, heads, origin, block_rows):
    group = lax.axis_index("fs") * lax.axis_size("tp") + lax.axis_index("tp")
    place = pl.multiple_of(jnp.maximum(origin, 0) * block_rows, block_rows)
    return gates_ref[pl.ds(group * heads + h, 1), pl.ds(place, block_rows)] * log2e


def score(queries, keys, gate_q, gate_k, origin):
    scale = queries.shape[1] ** (-0.5) * log2e
    s = lax.dot_general(
        queries, keys, (((1,), (1,)), ((), ())), preferred_element_type=f32
    )
    return s * scale + gate_q - jnp.where(origin >= 0, gate_k, -masked_score)


def early_kernel(*refs):
    q_ref, gates_ref, mask_ref = refs[:3]
    acc_ref, stat_ref, column_ref, key_ref, value_ref, natural_ref = refs[-6:]
    halves = refs[3:-6]
    place_pairs(tuple(zip(halves[::2], halves[1::2])), key_ref, value_ref)
    z = lax.axis_index("sp")
    block_rows = q_ref.shape[0]
    head_dim = key_ref.shape[1]
    heads = q_ref.shape[1] // head_dim
    origins = [z] + [z - k for k in range(2, len(halves) // 2 + 1)]
    n_fs = lax.axis_size("fs")
    step = block_rows // (2 * n_fs)
    places = row_places(n_fs, step)
    for h in range(heads):
        row = gate_row(gates_ref, h, heads, z, block_rows)
        natural_ref[...] = jnp.broadcast_to(row, (8, block_rows)).T
        for i, place in enumerate(places):
            column_ref[h, i * step : (i + 1) * step] = natural_ref[pl.ds(place, step)]
    tile = block_rows // 2
    masks = []
    for i in range(0, 2 * n_fs, n_fs):
        piece = [mask_ref[pl.ds(place, step)] for place in places[i : i + n_fs]]
        masks.append(jnp.concatenate(piece, axis=0))
    for h in range(heads):
        for i in range(0, block_rows, tile):
            queries = q_ref[i : i + tile, h * head_dim : (h + 1) * head_dim]
            gate_q = column_ref[h, i : i + tile, 0:1]
            scores = []
            for k, origin in enumerate(origins):
                gate_k = gate_row(gates_ref, h, heads, origin, block_rows)
                keys = key_ref[k * block_rows : (k + 1) * block_rows]
                s = score(queries, keys, gate_q, gate_k, origin)
                scores.append(s + masks[i // tile] if k == 0 else s)
            top = functools.reduce(jnp.maximum, scores)
            top = jnp.max(top, axis=1, keepdims=True)
            total = 0.0
            weighted = 0.0
            for k, s in enumerate(scores):
                weight = jnp.exp2(s - top)
                total = total + weight
                weighted = weighted + jnp.dot(
                    weight.astype(bf16),
                    value_ref[k * block_rows : (k + 1) * block_rows],
                    preferred_element_type=f32,
                )
            den = jnp.sum(total, axis=1, keepdims=True)
            place = h * block_rows + i
            acc_ref[place : place + tile] = weighted
            lane = lax.broadcasted_iota(jnp.int32, (tile, head_dim), 1)
            stat_ref[place : place + tile] = jnp.where(lane == 0, top, den)


def row_places(n_fs, step):
    f = lax.axis_index("fs")
    t = lax.axis_index("tp")
    return [
        pl.multiple_of((f ^ k) * 2 * step + lane * step, step)
        for lane in (1 - t, t)
        for k in range(n_fs - 1, -1, -1)
    ]


def project_kernel(n_fs, *refs):
    own, other = refs[:n_fs], refs[n_fs : 2 * n_fs]
    w_query, w_post, w_pre, w_conv, pair_ref = refs[2 * n_fs : 2 * n_fs + 5]
    q_ref, post_ref, mixed_ref, rise_ref = refs[2 * n_fs + 5 :]
    step = own[0].shape[0]
    rows = jnp.concatenate([ref[...] for ref in (*other[::-1], *own[::-1])], axis=0)
    weight = jnp.concatenate([w_pre[...], w_conv[...]], axis=1)
    gated = jnp.dot(rows, weight, preferred_element_type=f32).astype(bf16).astype(f32)
    channels = w_pre.shape[1]
    mixed = (gated[:, :channels] * gated[:, channels:]).astype(bf16)
    for i, place in enumerate(row_places(n_fs, step)):
        mixed_ref[pl.ds(place, step)] = mixed[i * step : (i + 1) * step]
    lane_rows = pair_ref.shape[0]
    rise_ref[:lane_rows] = pair_ref[...]
    last = mixed_ref[mixed_ref.shape[0] - EDGE :]
    rise_ref[lane_rows:] = jnp.concatenate([last] * (rise_ref.shape[1] // channels), axis=1)
    q_ref[...] = jnp.dot(rows, w_query[...], preferred_element_type=f32).astype(bf16)
    post_ref[...] = jnp.dot(rows, w_post[...], preferred_element_type=f32).astype(bf16)


def stack_kernel(top_ref, low_ref, out_ref):
    out_ref[: top_ref.shape[0]] = top_ref[...]
    out_ref[top_ref.shape[0] :] = low_ref[...]


def conv_kernel(n_fs, post_ref, mixed_ref, risen_ref, taps_ref, out_ref, extended_ref, sum_ref):
    block_rows, channels = mixed_ref.shape
    group = lax.axis_index("fs") * lax.axis_size("tp") + lax.axis_index("tp")
    lanes = pl.ds(pl.multiple_of(group * channels, channels), channels)
    taps = taps_ref.shape[0]
    halo = risen_ref[risen_ref.shape[0] - EDGE :, :channels].astype(f32)
    extended_ref[0:EDGE] = jnp.where(lax.axis_index("sp") > 0, halo, 0.0)
    extended_ref[EDGE:] = mixed_ref[...].astype(f32)
    tap_rows = taps_ref[:, lanes].astype(f32)
    first = EDGE - (taps - 1)
    conv_sum = tap_rows[0:1] * extended_ref[first : first + block_rows]
    for i in range(1, taps):
        conv_sum = conv_sum + tap_rows[i : i + 1] * extended_ref[first + i : first + i + block_rows]
    sum_ref[...] = conv_sum
    step = block_rows // (2 * n_fs)
    for i, place in enumerate(row_places(n_fs, step)):
        rows = slice(i * step, (i + 1) * step)
        out_ref[rows] = (post_ref[rows].astype(f32) * sum_ref[pl.ds(place, step)]).astype(bf16)


def mixer_kernel(first, *refs):
    q_ref, conv_ref, gates_ref, column_ref, acc_ref, stat_ref = refs[:6]
    near_ref, far_ref, weight_ref, out_ref, key_ref, value_ref = refs[6:]
    place_pairs(((near_ref, far_ref),), key_ref, value_ref)
    block_rows = q_ref.shape[0]
    head_dim = key_ref.shape[1]
    heads = q_ref.shape[1] // head_dim
    rows = out_ref.shape[0]
    origin = lax.axis_index("sp") - 1
    outs = [conv_ref[first : first + rows]]
    for h in range(heads):
        queries = q_ref[first : first + rows, h * head_dim : (h + 1) * head_dim]
        gate_q = column_ref[h, first : first + rows, 0:1]
        gate_k = gate_row(gates_ref, h, heads, origin, block_rows)
        s = score(queries, key_ref[...], gate_q, gate_k, origin)
        place = h * block_rows + first
        held_top = stat_ref[place : place + rows, 0:1]
        held_den = stat_ref[place : place + rows, 1:2]
        top = jnp.maximum(held_top, jnp.max(s, axis=1, keepdims=True))
        fade = jnp.exp2(held_top - top)
        weight = jnp.exp2(s - top)
        den = held_den * fade + jnp.sum(weight, axis=1, keepdims=True)
        weighted = jnp.dot(weight.astype(bf16), value_ref[...], preferred_element_type=f32)
        held = acc_ref[place : place + rows]
        outs.append(((held * fade + weighted) / den).astype(bf16))
    out = jnp.dot(jnp.concatenate(outs, axis=1), weight_ref[...], preferred_element_type=f32)
    out_ref[...] = out.astype(bf16)


def pair_sum_kernel(keep_ref, got_ref, *outs):
    step = outs[0].shape[0]
    for i, out in enumerate(outs):
        rows = slice(i * step, (i + 1) * step)
        total = keep_ref[rows].astype(f32) + got_ref[rows].astype(f32)
        out[...] = total.astype(out.dtype)


def final_kernel(*refs):
    total = refs[0][...].astype(f32)
    for ref in refs[1:-1]:
        total = total + ref[...].astype(f32)
    refs[-1][...] = total.astype(bf16)


def layer(
    tokens,
    norm_gain,
    w_query,
    w_key,
    w_value,
    w_conv_value,
    w_conv_pre,
    w_conv_post,
    conv_taps,
    log_gate_cache,
    w_out_conv,
    w_out_attn,
):
    n_sp, n_fs, n_tp = lax.axis_size("sp"), lax.axis_size("fs"), lax.axis_size("tp")
    step, width = tokens.shape
    lane_rows = n_fs * step
    block_rows = n_tp * lane_rows
    channels = w_conv_post.shape[1]
    head_dim = w_key.shape[1]
    heads = w_query.shape[1] // head_dim

    def swapped(x):
        return lax.ppermute(x, "tp", [(0, 1), (1, 0)])

    def crossed(x, k):
        return lax.ppermute(x, "fs", [(i, i ^ k) for i in range(n_fs)])

    def raised(x, shift):
        route = [(i, (i + shift) % n_sp) for i in range(n_sp) if i + shift < n_sp or RING]
        return lax.ppermute(x, "sp", route)

    def call(kernel, out_shape, scratch, mib, *operands, in_specs=None, work=0):
        extra = {} if in_specs is None else {"in_specs": in_specs}
        if work:
            extra["cost_estimate"] = pl.CostEstimate(
                flops=work, transcendentals=0, bytes_accessed=0
            )
        return pl.pallas_call(
            kernel,
            out_shape=out_shape,
            scratch_shapes=scratch,
            compiler_params=kernel_params(mib),
            **extra,
        )(*operands)

    mask = call(mask_kernel, shape_of(block_rows, block_rows, f32), [], 4, work=MASK_WORK)
    normed = call(
        norm_kernel,
        shape_of(step, width),
        [],
        4,
        tokens,
        norm_gain.reshape(1, width),
        work=NORM_WORK,
    )
    w_post, w_pre, w_conv = w_conv_post, w_conv_pre, w_conv_value
    gates, taps = log_gate_cache, conv_taps
    own = [normed] + [crossed(normed, k) for k in range(1, n_fs)]
    other = [swapped(x) for x in own]
    pair = call(
        functools.partial(pair_kernel, n_fs),
        shape_of(lane_rows, 2 * head_dim),
        [pltpu.VMEM((lane_rows, width), bf16)],
        8,
        *own,
        w_key,
        w_value,
        work=SMALL_WORK,
    )
    halves = [pair, swapped(pair)]
    for shift in range(2, n_sp):
        piece = raised(pair, shift)
        halves += [piece, swapped(piece)]
    queries, post, mixed, rise = call(
        functools.partial(project_kernel, n_fs),
        (
            shape_of(block_rows, heads * head_dim),
            shape_of(block_rows, channels),
            shape_of(block_rows, channels),
            shape_of(lane_rows + EDGE, 2 * head_dim),
        ),
        [],
        16,
        *own,
        *other,
        w_query,
        w_post,
        w_pre,
        w_conv,
        pair,
        work=SMALL_WORK,
    )
    near = raised(rise, 1)
    far = swapped(near)
    acc, stat, column = call(
        early_kernel,
        (
            shape_of(heads * block_rows, head_dim, f32),
            shape_of(heads * block_rows, head_dim, f32),
            jax.ShapeDtypeStruct((heads, block_rows, 8), f32),
        ),
        [pltpu.VMEM((len(halves) * lane_rows, head_dim), bf16)] * 2
        + [pltpu.VMEM((block_rows, 8), f32)],
        16,
        queries,
        gates,
        mask,
        *halves,
        work=SMALL_WORK,
    )
    conv_out = call(
        functools.partial(conv_kernel, n_fs),
        shape_of(block_rows, channels),
        [pltpu.VMEM((block_rows + EDGE, channels), f32), pltpu.VMEM((block_rows, channels), f32)],
        4,
        post,
        mixed,
        near,
        taps,
        work=SMALL_WORK,
    )
    w_out = call(
        stack_kernel,
        shape_of(w_out_conv.shape[0] + w_out_attn.shape[0], width),
        [],
        8,
        w_out_conv,
        w_out_attn,
    )

    def mixed_rows(first):
        return call(
            functools.partial(mixer_kernel, first),
            shape_of(lane_rows, width),
            [pltpu.VMEM((block_rows, head_dim), bf16)] * 2,
            16,
            queries,
            conv_out,
            gates,
            column,
            acc,
            stat,
            near,
            far,
            w_out,
            work=SMALL_WORK,
        )

    send = mixed_rows(0)
    got = swapped(send)
    keep = mixed_rows(lane_rows)
    parts = range(n_fs - 1, -1, -1)
    pieces = call(
        pair_sum_kernel,
        tuple(shape_of(step, width, bf16 if k else f32) for k in parts),
        [],
        8,
        keep,
        got,
    )
    sums = [crossed(piece, k) if k else piece for k, piece in zip(parts, pieces)]
    return call(final_kernel, shape_of(step, width), [], 4, *sums)


def passed_along(block, axis, distance):
    devices = range(lax.axis_size(axis))
    route = [(i - distance, i) for i in devices if i - distance in devices]
    return lax.ppermute(block, axis, route)


def shards(
    tokens,
    norm_gain,
    w_query,
    w_key,
    w_value,
    w_conv_value,
    w_conv_pre,
    w_conv_post,
    conv_taps,
    log_gate_cache,
    w_out_conv,
    w_out_attn,
):
    float_rows = tokens.astype(jnp.float32)
    scaled = float_rows * lax.rsqrt(
        jnp.mean(float_rows * float_rows, axis=1, keepdims=True) + epsilon
    )
    normed_own = (scaled * norm_gain).astype(jnp.bfloat16)
    normed = lax.all_gather(normed_own, ("fs", "tp"), axis=0, tiled=True)
    block_rows = normed.shape[0]
    channels = w_conv_post.shape[1]
    head_dim = w_key.shape[1]
    local_heads = w_query.shape[1] // head_dim
    group = lax.axis_index(("fs", "tp"))
    local_weight = jnp.concatenate([w_conv_post, w_conv_pre, w_conv_value, w_query], axis=1)
    projected = jnp.dot(normed, local_weight, preferred_element_type=jnp.float32).astype(
        jnp.bfloat16
    )
    post_gate = projected[:, :channels]
    pre_gate = projected[:, channels : 2 * channels]
    conv_value = projected[:, 2 * channels : 3 * channels]
    queries = projected[:, 3 * channels :].reshape(block_rows, local_heads, head_dim)
    mixed_in = (pre_gate.astype(jnp.float32) * conv_value.astype(jnp.float32)).astype(jnp.bfloat16)
    kernel = conv_taps.shape[0]
    carried = passed_along(mixed_in[block_rows - (kernel - 1) :], "sp", 1)
    extended = jnp.concatenate([carried, mixed_in], axis=0).astype(jnp.float32)
    tap_weights = lax.dynamic_slice_in_dim(conv_taps, group * channels, channels, 1).astype(
        jnp.float32
    )
    conv_sum = tap_weights[0] * extended[0:block_rows]
    for offset in range(1, kernel):
        conv_sum = conv_sum + tap_weights[offset] * extended[offset : offset + block_rows]
    conv_out = (post_gate.astype(jnp.float32) * conv_sum).astype(jnp.bfloat16)
    core_index = lax.axis_index("tp")
    half_rows = block_rows // 2
    own_rows = lax.dynamic_slice_in_dim(normed, core_index * half_rows, half_rows, 0)
    pair_weight = jnp.concatenate([w_key, w_value], axis=1)
    pair_rows = jnp.dot(own_rows, pair_weight, preferred_element_type=jnp.float32).astype(
        jnp.bfloat16
    )
    key_half = pair_rows[:, :head_dim]
    value_half = pair_rows[:, head_dim:]
    head_gates = lax.dynamic_slice_in_dim(log_gate_cache, group * local_heads, local_heads, 0)
    anchor = lax.axis_index("sp") * block_rows
    gate_query = lax.dynamic_slice_in_dim(head_gates, anchor, block_rows, 1).T
    sequence_places = anchor + lax.iota(jnp.int32, block_rows)
    score_scale = head_dim ** (-0.5)

    def absorb(carried_state, key_block, value_block, sub_start):
        running_max, running_sum, weighted = carried_state
        sub_width = key_block.shape[0]
        scores = (
            jnp.einsum("qhd,kd->qhk", queries, key_block, preferred_element_type=jnp.float32)
            * score_scale
        )
        gate_keys = lax.dynamic_slice_in_dim(head_gates, sub_start, sub_width, 1)
        scores = scores + gate_query[:, :, None] - gate_keys[None, :, :]
        key_positions = sub_start + lax.iota(jnp.int32, sub_width)
        scores = jnp.where(
            sequence_places[:, None, None] >= key_positions[None, None, :], scores, masked_score
        )
        new_max = jnp.maximum(running_max, jnp.max(scores, axis=2))
        rescale = jnp.exp(running_max - new_max)
        weights = jnp.exp(scores - new_max[:, :, None])
        running_sum = running_sum * rescale + jnp.sum(weights, axis=2)
        weighted = weighted * rescale[:, :, None] + jnp.einsum(
            "qhk,kd->qhd",
            weights.astype(jnp.bfloat16),
            value_block,
            preferred_element_type=jnp.float32,
        )
        return (new_max, running_sum, weighted)

    initial = (
        jnp.full((block_rows, local_heads), masked_score, jnp.float32),
        jnp.zeros((block_rows, local_heads), jnp.float32),
        jnp.zeros((block_rows, local_heads, head_dim), jnp.float32),
    )
    key_piece = lax.all_gather(key_half, ("sp", "tp"), axis=0, tiled=True)
    value_piece = lax.all_gather(value_half, ("sp", "tp"), axis=0, tiled=True)
    key_count = key_piece.shape[0]
    sub_width = 512

    def sweep_keys(current):

        def absorb_step(running, step_index):
            sub_start = step_index * sub_width
            key_block = lax.dynamic_slice_in_dim(key_piece, sub_start, sub_width, 0)
            value_block = lax.dynamic_slice_in_dim(value_piece, sub_start, sub_width, 0)
            return (absorb(running, key_block, value_block, sub_start), None)

        result, _ = lax.scan(
            absorb_step, current, jnp.arange(key_count // sub_width, dtype=jnp.int32)
        )
        return result

    def keep_state(current):
        return current

    _, running_sum, weighted = lax.cond(
        jnp.int32(0) <= anchor + block_rows - 1, sweep_keys, keep_state, initial
    )
    attn_out = (
        (weighted / running_sum[:, :, None])
        .astype(jnp.bfloat16)
        .reshape(block_rows, local_heads * head_dim)
    )
    return lax.psum_scatter(
        (
            jnp.dot(conv_out, w_out_conv, preferred_element_type=jnp.float32)
            + jnp.dot(attn_out, w_out_attn, preferred_element_type=jnp.float32)
        ).astype(jnp.bfloat16),
        ("fs", "tp"),
        scatter_dimension=0,
        tiled=True,
    )


def solution(mesh):
    few = mesh.shape["sp"] == 4
    placed = (
        P(("sp", "fs", "tp"), None),
        P(),
        P(None, ("fs", "tp")),
        P(None, "fs"),
        P(None, "fs"),
        P(None, ("fs", "tp")),
        P(None, ("fs", "tp")),
        P(None, ("fs", "tp")),
        P(),
        P(),
        P(("fs", "tp"), None),
        P(("fs", "tp"), None),
    )
    return jax.shard_map(
        layer if few else shards,
        mesh=mesh,
        in_specs=placed,
        out_specs=P(("sp", "fs", "tp"), None),
        check_vma=False,
    )
```

```python
import functools
import math
import jax
import jax.numpy as jnp
from jax import lax
from jax.experimental import pallas as pl
from jax.experimental.pallas import tpu as pltpu
from jax.sharding import PartitionSpec as P

epsilon = 1e-06
masked_score = -1e30
log2e = math.log2(math.e)
f32 = jnp.float32
bf16 = jnp.bfloat16
EDGE = 16
RING = (False, False, True, True)
NORM_WORK = 20000000000
MASK_WORK = 2000000000
SMALL_WORK = 2000000000


def kernel_params(mib):
    return pltpu.CompilerParams(vmem_limit_bytes=mib * 1024 * 1024)


def shape_of(rows, cols, dtype=bf16):
    return jax.ShapeDtypeStruct((rows, cols), dtype)


def mask_kernel(out_ref):
    query_place = lax.broadcasted_iota(jnp.int32, out_ref.shape, 0)
    key_place = lax.broadcasted_iota(jnp.int32, out_ref.shape, 1)
    out_ref[...] = jnp.where(query_place >= key_place, 0.0, masked_score)


def norm_kernel(tokens_ref, gain_ref, out_ref):
    rows = tokens_ref[...].astype(f32)
    scale = lax.rsqrt(jnp.mean(rows * rows, axis=1, keepdims=True) + epsilon)
    out_ref[...] = (rows * scale * gain_ref[...]).astype(bf16)


def pair_kernel(n_fs, *refs):
    chunks, (w_key, w_value, out_ref, rows_ref) = refs[:n_fs], refs[n_fs:]
    step = chunks[0].shape[0]
    f = lax.axis_index("fs")
    for k in range(n_fs):
        rows_ref[pl.ds(pl.multiple_of((f ^ k) * step, step), step)] = chunks[k][...]
    weight = jnp.concatenate([w_key[...], w_value[...]], axis=1)
    out_ref[...] = jnp.dot(rows_ref[...], weight, preferred_element_type=f32).astype(bf16)


def place_pairs(pieces, key_ref, value_ref):
    head_dim = key_ref.shape[1]
    t = lax.axis_index("tp")
    n_fs = lax.axis_size("fs")
    step = key_ref.shape[0] // (2 * n_fs * len(pieces))
    for k, (near, far) in enumerate(pieces):
        for lane, piece in ((t, near), (1 - t, far)):
            for g in range(n_fs):
                place = (k * n_fs + g) * 2 * step + lane * step
                place = pl.ds(pl.multiple_of(place, step), step)
                key_ref[place] = piece[g * step : (g + 1) * step, :head_dim]
                value_ref[place] = piece[g * step : (g + 1) * step, head_dim:]


def gate_row(gates_ref, h, heads, origin, block_rows):
    group = lax.axis_index("fs") * lax.axis_size("tp") + lax.axis_index("tp")
    place = pl.multiple_of(jnp.maximum(origin, 0) * block_rows, block_rows)
    return gates_ref[pl.ds(group * heads + h, 1), pl.ds(place, block_rows)] * log2e


def score(queries, keys, gate_q, gate_k, origin):
    scale = queries.shape[1] ** (-0.5) * log2e
    s = lax.dot_general(
        queries, keys, (((1,), (1,)), ((), ())), preferred_element_type=f32
    )
    return s * scale + gate_q - jnp.where(origin >= 0, gate_k, -masked_score)


def fold_blocks(q_ref, gates_ref, column_ref, blocks, masks, acc_ref, stat_ref):
    block_rows = q_ref.shape[0]
    head_dim = acc_ref.shape[1]
    heads = q_ref.shape[1] // head_dim
    tile = block_rows // 2
    for h in range(heads):
        for i in range(0, block_rows, tile):
            queries = q_ref[i : i + tile, h * head_dim : (h + 1) * head_dim]
            gate_q = column_ref[h, i : i + tile, 0:1]
            scores = []
            for k, (keys, values, origin) in enumerate(blocks):
                gate_k = gate_row(gates_ref, h, heads, origin, block_rows)
                s = score(queries, keys, gate_q, gate_k, origin)
                scores.append(s if k else s + masks[i // tile])
            top = jnp.max(functools.reduce(jnp.maximum, scores), axis=1, keepdims=True)
            weights = [jnp.exp2(s - top) for s in scores]
            den = jnp.sum(sum(weights), axis=1, keepdims=True)
            weighted = sum(
                jnp.dot(weight.astype(bf16), values, preferred_element_type=f32)
                for weight, (keys, values, origin) in zip(weights, blocks)
            )
            place = slice(h * block_rows + i, h * block_rows + i + tile)
            acc_ref[place] = weighted
            lane = lax.broadcasted_iota(jnp.int32, (tile, head_dim), 1)
            stat_ref[place] = jnp.where(lane == 0, top, den)


def early_kernel(*refs):
    q_ref, gates_ref, mask_ref = refs[:3]
    acc_ref, stat_ref, column_ref, key_ref, value_ref, natural_ref = refs[-6:]
    pieces = tuple(zip(refs[3:-6:2], refs[4:-6:2]))
    z = lax.axis_index("sp")
    block_rows = q_ref.shape[0]
    heads = column_ref.shape[0]
    n_fs = lax.axis_size("fs")
    step = block_rows // (2 * n_fs)
    places = row_places(n_fs, step)
    for h in range(heads):
        row = gate_row(gates_ref, h, heads, z, block_rows)
        natural_ref[...] = jnp.broadcast_to(row, (8, block_rows)).T
        for i, place in enumerate(places):
            column_ref[h, i * step : (i + 1) * step] = natural_ref[pl.ds(place, step)]

    def fold(count):
        masks = []
        for i in range(0, 2 * n_fs, n_fs):
            piece = [mask_ref[pl.ds(place, step)] for place in places[i : i + n_fs]]
            masks.append(jnp.concatenate(piece, axis=0))
        rows = slice(0, count * block_rows)
        place_pairs(pieces[:count], key_ref.at[rows], value_ref.at[rows])
        blocks = []
        for k in range(count):
            rows = slice(k * block_rows, (k + 1) * block_rows)
            blocks.append((key_ref[rows], value_ref[rows], z - k - min(k, 1)))
        fold_blocks(q_ref, gates_ref, column_ref, blocks, masks, acc_ref, stat_ref)

    for count in range(1, len(pieces) + 1):
        pl.when(jnp.maximum(z, 1) == count)(functools.partial(fold, count))


def row_places(n_fs, step):
    f = lax.axis_index("fs")
    t = lax.axis_index("tp")
    return [
        pl.multiple_of((f ^ k) * 2 * step + lane * step, step)
        for lane in (1 - t, t)
        for k in range(n_fs - 1, -1, -1)
    ]


def project_kernel(n_fs, *refs):
    own, other = refs[:n_fs], refs[n_fs : 2 * n_fs]
    w_query, w_post, w_pre, w_conv, pair_ref = refs[2 * n_fs : 2 * n_fs + 5]
    q_ref, post_ref, mixed_ref, rise_ref = refs[2 * n_fs + 5 :]
    step = own[0].shape[0]
    rows = jnp.concatenate([ref[...] for ref in (*other[::-1], *own[::-1])], axis=0)
    weight = jnp.concatenate([w_pre[...], w_conv[...]], axis=1)
    gated = jnp.dot(rows, weight, preferred_element_type=f32).astype(bf16).astype(f32)
    channels = w_pre.shape[1]
    mixed = (gated[:, :channels] * gated[:, channels:]).astype(bf16)
    for i, place in enumerate(row_places(n_fs, step)):
        mixed_ref[pl.ds(place, step)] = mixed[i * step : (i + 1) * step]
    lane_rows = pair_ref.shape[0]
    rise_ref[:lane_rows] = pair_ref[...]
    last = mixed_ref[mixed_ref.shape[0] - EDGE :]
    rise_ref[lane_rows:] = jnp.concatenate([last] * (rise_ref.shape[1] // channels), axis=1)
    q_ref[...] = jnp.dot(rows, w_query[...], preferred_element_type=f32).astype(bf16)
    post_ref[...] = jnp.dot(rows, w_post[...], preferred_element_type=f32).astype(bf16)


def stack_kernel(top_ref, low_ref, out_ref):
    out_ref[: top_ref.shape[0]] = top_ref[...]
    out_ref[top_ref.shape[0] :] = low_ref[...]


def conv_kernel(n_fs, post_ref, mixed_ref, risen_ref, taps_ref, out_ref, extended_ref, sum_ref):
    block_rows, channels = mixed_ref.shape
    group = lax.axis_index("fs") * lax.axis_size("tp") + lax.axis_index("tp")
    lanes = pl.ds(pl.multiple_of(group * channels, channels), channels)
    taps = taps_ref.shape[0]
    halo = risen_ref[risen_ref.shape[0] - EDGE :, :channels].astype(f32)
    extended_ref[0:EDGE] = jnp.where(lax.axis_index("sp") > 0, halo, 0.0)
    extended_ref[EDGE:] = mixed_ref[...].astype(f32)
    tap_rows = taps_ref[:, lanes].astype(f32)
    first = EDGE - (taps - 1)
    conv_sum = tap_rows[0:1] * extended_ref[first : first + block_rows]
    for i in range(1, taps):
        conv_sum = conv_sum + tap_rows[i : i + 1] * extended_ref[first + i : first + i + block_rows]
    sum_ref[...] = conv_sum
    step = block_rows // (2 * n_fs)
    for i, place in enumerate(row_places(n_fs, step)):
        rows = slice(i * step, (i + 1) * step)
        out_ref[rows] = (post_ref[rows].astype(f32) * sum_ref[pl.ds(place, step)]).astype(bf16)


def mixer_kernel(first, *refs):
    q_ref, conv_ref, gates_ref, column_ref, acc_ref, stat_ref = refs[:6]
    near_ref, far_ref, weight_ref, out_ref, key_ref, value_ref, row_ref = refs[6:]
    block_rows = q_ref.shape[0]
    head_dim = key_ref.shape[1]
    channels = conv_ref.shape[1]
    heads = q_ref.shape[1] // head_dim
    rows = out_ref.shape[0]
    origin = lax.axis_index("sp") - 1
    row_ref[:, :channels] = conv_ref[first : first + rows]

    def put(h, value):
        place = channels + h * head_dim
        row_ref[:, place : place + head_dim] = value.astype(bf16)

    @pl.when(origin < 0)
    def alone():
        for h in range(heads):
            place = h * block_rows + first
            put(h, acc_ref[place : place + rows] / stat_ref[place : place + rows, 1:2])

    @pl.when(origin >= 0)
    def joined():
        place_pairs(((near_ref, far_ref),), key_ref, value_ref)
        for h in range(heads):
            queries = q_ref[first : first + rows, h * head_dim : (h + 1) * head_dim]
            gate_q = column_ref[h, first : first + rows, 0:1]
            gate_k = gate_row(gates_ref, h, heads, origin, block_rows)
            s = score(queries, key_ref[...], gate_q, gate_k, origin)
            place = h * block_rows + first
            held_top = stat_ref[place : place + rows, 0:1]
            held_den = stat_ref[place : place + rows, 1:2]
            top = jnp.maximum(held_top, jnp.max(s, axis=1, keepdims=True))
            fade = jnp.exp2(held_top - top)
            weight = jnp.exp2(s - top)
            den = held_den * fade + jnp.sum(weight, axis=1, keepdims=True)
            weighted = jnp.dot(weight.astype(bf16), value_ref[...], preferred_element_type=f32)
            put(h, (acc_ref[place : place + rows] * fade + weighted) / den)

    out = jnp.dot(row_ref[...], weight_ref[...], preferred_element_type=f32)
    out_ref[...] = out.astype(bf16)


def pair_sum_kernel(keep_ref, got_ref, *outs):
    step = outs[0].shape[0]
    for i, out in enumerate(outs):
        rows = slice(i * step, (i + 1) * step)
        total = keep_ref[rows].astype(f32) + got_ref[rows].astype(f32)
        out[...] = total.astype(out.dtype)


def final_kernel(*refs):
    total = refs[0][...].astype(f32)
    for ref in refs[1:-1]:
        total = total + ref[...].astype(f32)
    refs[-1][...] = total.astype(bf16)


def layer(
    tokens,
    norm_gain,
    w_query,
    w_key,
    w_value,
    w_conv_value,
    w_conv_pre,
    w_conv_post,
    conv_taps,
    log_gate_cache,
    w_out_conv,
    w_out_attn,
):
    n_sp, n_fs, n_tp = lax.axis_size("sp"), lax.axis_size("fs"), lax.axis_size("tp")
    step, width = tokens.shape
    lane_rows = n_fs * step
    block_rows = n_tp * lane_rows
    channels = w_conv_post.shape[1]
    head_dim = w_key.shape[1]
    heads = w_query.shape[1] // head_dim

    def swapped(x):
        return lax.ppermute(x, "tp", [(0, 1), (1, 0)])

    def crossed(x, k):
        return lax.ppermute(x, "fs", [(i, i ^ k) for i in range(n_fs)])

    def raised(x, shift):
        route = [(i, (i + shift) % n_sp) for i in range(n_sp) if i + shift < n_sp or RING[shift]]
        return lax.ppermute(x, "sp", route)

    def call(kernel, out_shape, scratch, mib, *operands, in_specs=None, work=0):
        extra = {} if in_specs is None else {"in_specs": in_specs}
        if work:
            extra["cost_estimate"] = pl.CostEstimate(
                flops=work, transcendentals=0, bytes_accessed=0
            )
        return pl.pallas_call(
            kernel,
            out_shape=out_shape,
            scratch_shapes=scratch,
            compiler_params=kernel_params(mib),
            **extra,
        )(*operands)

    mask = call(mask_kernel, shape_of(block_rows, block_rows, f32), [], 4, work=MASK_WORK)
    normed = call(
        norm_kernel,
        shape_of(step, width),
        [],
        4,
        tokens,
        norm_gain.reshape(1, width),
        work=NORM_WORK,
    )
    w_post, w_pre, w_conv = w_conv_post, w_conv_pre, w_conv_value
    gates, taps = log_gate_cache, conv_taps
    own = [normed] + [crossed(normed, k) for k in range(1, n_fs)]
    other = [swapped(x) for x in own]
    pair = call(
        functools.partial(pair_kernel, n_fs),
        shape_of(lane_rows, 2 * head_dim),
        [pltpu.VMEM((lane_rows, width), bf16)],
        8,
        *own,
        w_key,
        w_value,
        work=SMALL_WORK,
    )
    halves = [pair, swapped(pair)]
    for shift in range(2, n_sp):
        piece = raised(pair, shift)
        halves += [piece, swapped(piece)]
    queries, post, mixed, rise = call(
        functools.partial(project_kernel, n_fs),
        (
            shape_of(block_rows, heads * head_dim),
            shape_of(block_rows, channels),
            shape_of(block_rows, channels),
            shape_of(lane_rows + EDGE, 2 * head_dim),
        ),
        [],
        16,
        *own,
        *other,
        w_query,
        w_post,
        w_pre,
        w_conv,
        pair,
        work=SMALL_WORK,
    )
    near = raised(rise, 1)
    far = swapped(near)
    acc, stat, column = call(
        early_kernel,
        (
            shape_of(heads * block_rows, head_dim, f32),
            shape_of(heads * block_rows, head_dim, f32),
            jax.ShapeDtypeStruct((heads, block_rows, 8), f32),
        ),
        [pltpu.VMEM((len(halves) * lane_rows, head_dim), bf16)] * 2
        + [pltpu.VMEM((block_rows, 8), f32)],
        16,
        queries,
        gates,
        mask,
        *halves,
        work=SMALL_WORK,
    )
    conv_out = call(
        functools.partial(conv_kernel, n_fs),
        shape_of(block_rows, channels),
        [pltpu.VMEM((block_rows + EDGE, channels), f32), pltpu.VMEM((block_rows, channels), f32)],
        4,
        post,
        mixed,
        near,
        taps,
        work=SMALL_WORK,
    )
    w_out = call(
        stack_kernel,
        shape_of(w_out_conv.shape[0] + w_out_attn.shape[0], width),
        [],
        8,
        w_out_conv,
        w_out_attn,
    )

    def mixed_rows(first):
        return call(
            functools.partial(mixer_kernel, first),
            shape_of(lane_rows, width),
            [pltpu.VMEM((block_rows, head_dim), bf16)] * 2
            + [pltpu.VMEM((lane_rows, channels + heads * head_dim), bf16)],
            16,
            queries,
            conv_out,
            gates,
            column,
            acc,
            stat,
            near,
            far,
            w_out,
            work=SMALL_WORK,
        )

    send = mixed_rows(0)
    got = swapped(send)
    keep = mixed_rows(lane_rows)
    parts = range(n_fs - 1, -1, -1)
    pieces = call(
        pair_sum_kernel,
        tuple(shape_of(step, width, bf16 if k else f32) for k in parts),
        [],
        8,
        keep,
        got,
    )
    sums = [crossed(piece, k) if k else piece for k, piece in zip(parts, pieces)]
    return call(final_kernel, shape_of(step, width), [], 4, *sums)


def passed_along(block, axis, distance):
    devices = range(lax.axis_size(axis))
    route = [(i - distance, i) for i in devices if i - distance in devices]
    return lax.ppermute(block, axis, route)


def shards(
    tokens,
    norm_gain,
    w_query,
    w_key,
    w_value,
    w_conv_value,
    w_conv_pre,
    w_conv_post,
    conv_taps,
    log_gate_cache,
    w_out_conv,
    w_out_attn,
):
    float_rows = tokens.astype(jnp.float32)
    scaled = float_rows * lax.rsqrt(
        jnp.mean(float_rows * float_rows, axis=1, keepdims=True) + epsilon
    )
    normed_own = (scaled * norm_gain).astype(jnp.bfloat16)
    normed = lax.all_gather(normed_own, ("fs", "tp"), axis=0, tiled=True)
    block_rows = normed.shape[0]
    channels = w_conv_post.shape[1]
    head_dim = w_key.shape[1]
    local_heads = w_query.shape[1] // head_dim
    group = lax.axis_index(("fs", "tp"))
    local_weight = jnp.concatenate([w_conv_post, w_conv_pre, w_conv_value, w_query], axis=1)
    projected = jnp.dot(normed, local_weight, preferred_element_type=jnp.float32).astype(
        jnp.bfloat16
    )
    post_gate = projected[:, :channels]
    pre_gate = projected[:, channels : 2 * channels]
    conv_value = projected[:, 2 * channels : 3 * channels]
    queries = projected[:, 3 * channels :].reshape(block_rows, local_heads, head_dim)
    mixed_in = (pre_gate.astype(jnp.float32) * conv_value.astype(jnp.float32)).astype(jnp.bfloat16)
    kernel = conv_taps.shape[0]
    carried = passed_along(mixed_in[block_rows - (kernel - 1) :], "sp", 1)
    extended = jnp.concatenate([carried, mixed_in], axis=0).astype(jnp.float32)
    tap_weights = lax.dynamic_slice_in_dim(conv_taps, group * channels, channels, 1).astype(
        jnp.float32
    )
    conv_sum = tap_weights[0] * extended[0:block_rows]
    for offset in range(1, kernel):
        conv_sum = conv_sum + tap_weights[offset] * extended[offset : offset + block_rows]
    conv_out = (post_gate.astype(jnp.float32) * conv_sum).astype(jnp.bfloat16)
    core_index = lax.axis_index("tp")
    half_rows = block_rows // 2
    own_rows = lax.dynamic_slice_in_dim(normed, core_index * half_rows, half_rows, 0)
    pair_weight = jnp.concatenate([w_key, w_value], axis=1)
    pair_rows = jnp.dot(own_rows, pair_weight, preferred_element_type=jnp.float32).astype(
        jnp.bfloat16
    )
    key_half = pair_rows[:, :head_dim]
    value_half = pair_rows[:, head_dim:]
    head_gates = lax.dynamic_slice_in_dim(log_gate_cache, group * local_heads, local_heads, 0)
    anchor = lax.axis_index("sp") * block_rows
    gate_query = lax.dynamic_slice_in_dim(head_gates, anchor, block_rows, 1).T
    sequence_places = anchor + lax.iota(jnp.int32, block_rows)
    score_scale = head_dim ** (-0.5)

    def absorb(carried_state, key_block, value_block, sub_start):
        running_max, running_sum, weighted = carried_state
        sub_width = key_block.shape[0]
        scores = (
            jnp.einsum("qhd,kd->qhk", queries, key_block, preferred_element_type=jnp.float32)
            * score_scale
        )
        gate_keys = lax.dynamic_slice_in_dim(head_gates, sub_start, sub_width, 1)
        scores = scores + gate_query[:, :, None] - gate_keys[None, :, :]
        key_positions = sub_start + lax.iota(jnp.int32, sub_width)
        scores = jnp.where(
            sequence_places[:, None, None] >= key_positions[None, None, :], scores, masked_score
        )
        new_max = jnp.maximum(running_max, jnp.max(scores, axis=2))
        rescale = jnp.exp(running_max - new_max)
        weights = jnp.exp(scores - new_max[:, :, None])
        running_sum = running_sum * rescale + jnp.sum(weights, axis=2)
        weighted = weighted * rescale[:, :, None] + jnp.einsum(
            "qhk,kd->qhd",
            weights.astype(jnp.bfloat16),
            value_block,
            preferred_element_type=jnp.float32,
        )
        return (new_max, running_sum, weighted)

    initial = (
        jnp.full((block_rows, local_heads), masked_score, jnp.float32),
        jnp.zeros((block_rows, local_heads), jnp.float32),
        jnp.zeros((block_rows, local_heads, head_dim), jnp.float32),
    )
    key_piece = lax.all_gather(key_half, ("sp", "tp"), axis=0, tiled=True)
    value_piece = lax.all_gather(value_half, ("sp", "tp"), axis=0, tiled=True)
    key_count = key_piece.shape[0]
    sub_width = 512

    def sweep_keys(current):

        def absorb_step(running, step_index):
            sub_start = step_index * sub_width
            key_block = lax.dynamic_slice_in_dim(key_piece, sub_start, sub_width, 0)
            value_block = lax.dynamic_slice_in_dim(value_piece, sub_start, sub_width, 0)
            return (absorb(running, key_block, value_block, sub_start), None)

        result, _ = lax.scan(
            absorb_step, current, jnp.arange(key_count // sub_width, dtype=jnp.int32)
        )
        return result

    def keep_state(current):
        return current

    _, running_sum, weighted = lax.cond(
        jnp.int32(0) <= anchor + block_rows - 1, sweep_keys, keep_state, initial
    )
    attn_out = (
        (weighted / running_sum[:, :, None])
        .astype(jnp.bfloat16)
        .reshape(block_rows, local_heads * head_dim)
    )
    return lax.psum_scatter(
        (
            jnp.dot(conv_out, w_out_conv, preferred_element_type=jnp.float32)
            + jnp.dot(attn_out, w_out_attn, preferred_element_type=jnp.float32)
        ).astype(jnp.bfloat16),
        ("fs", "tp"),
        scatter_dimension=0,
        tiled=True,
    )


def solution(mesh):
    few = mesh.shape["sp"] == 4
    placed = (
        P(("sp", "fs", "tp"), None),
        P(),
        P(None, ("fs", "tp")),
        P(None, "fs"),
        P(None, "fs"),
        P(None, ("fs", "tp")),
        P(None, ("fs", "tp")),
        P(None, ("fs", "tp")),
        P(),
        P(),
        P(("fs", "tp"), None),
        P(("fs", "tp"), None),
    )
    return jax.shard_map(
        layer if few else shards,
        mesh=mesh,
        in_specs=placed,
        out_specs=P(("sp", "fs", "tp"), None),
        check_vma=False,
    )
```

```python
import functools
import math
import jax
import jax.numpy as jnp
from jax import lax
from jax.experimental import pallas as pl
from jax.experimental.pallas import tpu as pltpu
from jax.sharding import PartitionSpec as P

epsilon = 1e-06
masked_score = -1e30
log2e = math.log2(math.e)
f32 = jnp.float32
bf16 = jnp.bfloat16
EDGE = 16
RING = (False, False, True, True)
NORM_WORK = 20000000000
MASK_WORK = 2000000000
SMALL_WORK = 2000000000


def kernel_params(mib):
    return pltpu.CompilerParams(vmem_limit_bytes=mib * 1024 * 1024)


def shape_of(rows, cols, dtype=bf16):
    return jax.ShapeDtypeStruct((rows, cols), dtype)


def mask_kernel(out_ref):
    query_place = lax.broadcasted_iota(jnp.int32, out_ref.shape, 0)
    key_place = lax.broadcasted_iota(jnp.int32, out_ref.shape, 1)
    out_ref[...] = jnp.where(query_place >= key_place, 0.0, masked_score)


def norm_kernel(tokens_ref, gain_ref, out_ref):
    rows = tokens_ref[...].astype(f32)
    scale = lax.rsqrt(jnp.mean(rows * rows, axis=1, keepdims=True) + epsilon)
    out_ref[...] = (rows * scale * gain_ref[...]).astype(bf16)


def pair_kernel(n_fs, *refs):
    chunks, (w_key, w_value, out_ref, rows_ref) = refs[:n_fs], refs[n_fs:]
    step = chunks[0].shape[0]
    f = lax.axis_index("fs")
    for k in range(n_fs):
        rows_ref[pl.ds(pl.multiple_of((f ^ k) * step, step), step)] = chunks[k][...]
    weight = jnp.concatenate([w_key[...], w_value[...]], axis=1)
    out_ref[...] = jnp.dot(rows_ref[...], weight, preferred_element_type=f32).astype(bf16)


def place_pairs(pieces, key_ref, value_ref):
    head_dim = key_ref.shape[1]
    t = lax.axis_index("tp")
    n_fs = lax.axis_size("fs")
    step = key_ref.shape[0] // (2 * n_fs * len(pieces))
    for k, (near, far) in enumerate(pieces):
        for lane, piece in ((t, near), (1 - t, far)):
            for g in range(n_fs):
                place = (k * n_fs + g) * 2 * step + lane * step
                place = pl.ds(pl.multiple_of(place, step), step)
                key_ref[place] = piece[g * step : (g + 1) * step, :head_dim]
                value_ref[place] = piece[g * step : (g + 1) * step, head_dim:]


def gate_row(gates_ref, h, heads, origin, block_rows):
    group = lax.axis_index("fs") * lax.axis_size("tp") + lax.axis_index("tp")
    place = pl.multiple_of(jnp.maximum(origin, 0) * block_rows, block_rows)
    return gates_ref[pl.ds(group * heads + h, 1), pl.ds(place, block_rows)] * log2e


def score(queries, keys, gate_q, gate_k, origin):
    scale = queries.shape[1] ** (-0.5) * log2e
    s = lax.dot_general(
        queries, keys, (((1,), (1,)), ((), ())), preferred_element_type=f32
    )
    return s * scale + gate_q - jnp.where(origin >= 0, gate_k, -masked_score)


def faded(s, top):
    return jnp.exp2(s - jnp.concatenate([top] * (s.shape[1] // top.shape[1]), axis=1))


def fold_blocks(q_ref, gates_ref, column_ref, blocks, masks, held, outs):
    acc_ref, top_ref, den_ref = outs
    block_rows = q_ref.shape[0]
    head_dim = acc_ref.shape[1]
    heads = q_ref.shape[1] // head_dim
    tile = block_rows // 2
    tiles = [(h, i) for h in range(heads) for i in range(0, block_rows, tile)]
    places = [slice(h * block_rows + i, h * block_rows + i + tile) for h, i in tiles]
    scores = []
    for h, i in tiles:
        queries = q_ref[i : i + tile, h * head_dim : (h + 1) * head_dim]
        gate_q = column_ref[h, i : i + tile, 0:1]
        row = []
        for keys, values, origin in blocks:
            gate_k = gate_row(gates_ref, h, heads, origin, block_rows)
            s = score(queries, keys, gate_q, gate_k, origin)
            row.append(s + masks[i // tile] if masks else s)
        scores.append(row)
    wide = (tile, head_dim)
    tops = [
        jnp.broadcast_to(
            jnp.max(functools.reduce(jnp.maximum, row), axis=1, keepdims=True), wide
        )
        for row in scores
    ]
    if held:
        held_tops = [held[1][place] for place in places]
        tops = [jnp.maximum(top, held_top) for top, held_top in zip(tops, held_tops)]
        fades = [jnp.exp2(held_top - top) for top, held_top in zip(tops, held_tops)]
    weights = [[faded(s, top) for s in row] for row, top in zip(scores, tops)]
    dens = [
        jnp.broadcast_to(jnp.sum(sum(row), axis=1, keepdims=True), wide) for row in weights
    ]
    for n, place in enumerate(places):
        total = sum(
            jnp.dot(weight.astype(bf16), values, preferred_element_type=f32)
            for weight, (keys, values, origin) in zip(weights[n], blocks)
        )
        den = dens[n]
        if held:
            total = total + held[0][place] * fades[n]
            den = den + held[2][place] * fades[n]
        acc_ref[place] = total
        top_ref[place] = tops[n]
        den_ref[place] = den


def early_kernel(*refs):
    q_ref, gates_ref, mask_ref, near_ref, far_ref = refs[:5]
    outs, (column_ref, key_ref, value_ref, natural_ref) = refs[5:8], refs[8:]
    place_pairs(((near_ref, far_ref),), key_ref, value_ref)
    z = lax.axis_index("sp")
    block_rows = q_ref.shape[0]
    heads = column_ref.shape[0]
    n_fs = lax.axis_size("fs")
    step = block_rows // (2 * n_fs)
    places = row_places(n_fs, step)
    for h in range(heads):
        row = gate_row(gates_ref, h, heads, z, block_rows)
        natural_ref[...] = jnp.broadcast_to(row, (8, block_rows)).T
        for i, place in enumerate(places):
            column_ref[h, i * step : (i + 1) * step] = natural_ref[pl.ds(place, step)]
    masks = []
    for i in range(0, 2 * n_fs, n_fs):
        piece = [mask_ref[pl.ds(place, step)] for place in places[i : i + n_fs]]
        masks.append(jnp.concatenate(piece, axis=0))
    blocks = [(key_ref[...], value_ref[...], z)]
    fold_blocks(q_ref, gates_ref, column_ref, blocks, masks, None, outs)


def later_kernel(*refs):
    q_ref, gates_ref, column_ref = refs[:3]
    held, outs, (key_ref, value_ref) = refs[3:6], refs[-5:-2], refs[-2:]
    pieces = tuple(zip(refs[6:-5:2], refs[7:-5:2]))
    z = lax.axis_index("sp")
    block_rows = q_ref.shape[0]

    def keep():
        for source, out in zip(held, outs):
            out[...] = source[...]

    def fold(count):
        rows = slice(0, count * block_rows)
        place_pairs(pieces[:count], key_ref.at[rows], value_ref.at[rows])
        blocks = []
        for k in range(count):
            rows = slice(k * block_rows, (k + 1) * block_rows)
            blocks.append((key_ref[rows], value_ref[rows], z - 2 - k))
        fold_blocks(q_ref, gates_ref, column_ref, blocks, None, held, outs)

    pl.when(z < 2)(keep)
    for count in range(1, len(pieces) + 1):
        pl.when(z - 1 == count)(functools.partial(fold, count))


def row_places(n_fs, step):
    f = lax.axis_index("fs")
    t = lax.axis_index("tp")
    return [
        pl.multiple_of((f ^ k) * 2 * step + lane * step, step)
        for lane in (1 - t, t)
        for k in range(n_fs - 1, -1, -1)
    ]


def project_kernel(n_fs, *refs):
    own, other = refs[:n_fs], refs[n_fs : 2 * n_fs]
    w_query, w_post, w_pre, w_conv, pair_ref = refs[2 * n_fs : 2 * n_fs + 5]
    q_ref, post_ref, mixed_ref, rise_ref = refs[2 * n_fs + 5 :]
    step = own[0].shape[0]
    rows = jnp.concatenate([ref[...] for ref in (*other[::-1], *own[::-1])], axis=0)
    weight = jnp.concatenate([w_pre[...], w_conv[...]], axis=1)
    gated = jnp.dot(rows, weight, preferred_element_type=f32).astype(bf16).astype(f32)
    channels = w_pre.shape[1]
    mixed = (gated[:, :channels] * gated[:, channels:]).astype(bf16)
    for i, place in enumerate(row_places(n_fs, step)):
        mixed_ref[pl.ds(place, step)] = mixed[i * step : (i + 1) * step]
    lane_rows = pair_ref.shape[0]
    rise_ref[:lane_rows] = pair_ref[...]
    last = mixed_ref[mixed_ref.shape[0] - EDGE :]
    rise_ref[lane_rows:] = jnp.concatenate([last] * (rise_ref.shape[1] // channels), axis=1)
    q_ref[...] = jnp.dot(rows, w_query[...], preferred_element_type=f32).astype(bf16)
    post_ref[...] = jnp.dot(rows, w_post[...], preferred_element_type=f32).astype(bf16)


def stack_kernel(top_ref, low_ref, out_ref):
    out_ref[: top_ref.shape[0]] = top_ref[...]
    out_ref[top_ref.shape[0] :] = low_ref[...]


def conv_kernel(n_fs, post_ref, mixed_ref, risen_ref, taps_ref, out_ref, extended_ref, sum_ref):
    block_rows, channels = mixed_ref.shape
    group = lax.axis_index("fs") * lax.axis_size("tp") + lax.axis_index("tp")
    lanes = pl.ds(pl.multiple_of(group * channels, channels), channels)
    taps = taps_ref.shape[0]
    halo = risen_ref[risen_ref.shape[0] - EDGE :, :channels].astype(f32)
    extended_ref[0:EDGE] = jnp.where(lax.axis_index("sp") > 0, halo, 0.0)
    extended_ref[EDGE:] = mixed_ref[...].astype(f32)
    tap_rows = taps_ref[:, lanes].astype(f32)
    first = EDGE - (taps - 1)
    conv_sum = tap_rows[0:1] * extended_ref[first : first + block_rows]
    for i in range(1, taps):
        conv_sum = conv_sum + tap_rows[i : i + 1] * extended_ref[first + i : first + i + block_rows]
    sum_ref[...] = conv_sum
    step = block_rows // (2 * n_fs)
    for i, place in enumerate(row_places(n_fs, step)):
        rows = slice(i * step, (i + 1) * step)
        out_ref[rows] = (post_ref[rows].astype(f32) * sum_ref[pl.ds(place, step)]).astype(bf16)


def mixer_kernel(first, *refs):
    q_ref, conv_ref, gates_ref, column_ref, acc_ref, top_ref, den_ref = refs[:7]
    near_ref, far_ref, weight_ref, out_ref, key_ref, value_ref, row_ref = refs[7:]
    block_rows = q_ref.shape[0]
    head_dim = key_ref.shape[1]
    channels = conv_ref.shape[1]
    heads = q_ref.shape[1] // head_dim
    rows = out_ref.shape[0]
    origin = lax.axis_index("sp") - 1
    row_ref[:, :channels] = conv_ref[first : first + rows]

    def put(h, value):
        place = channels + h * head_dim
        row_ref[:, place : place + head_dim] = value.astype(bf16)

    @pl.when(origin < 0)
    def alone():
        for h in range(heads):
            place = h * block_rows + first
            put(h, acc_ref[place : place + rows] / den_ref[place : place + rows])

    @pl.when(origin >= 0)
    def joined():
        place_pairs(((near_ref, far_ref),), key_ref, value_ref)
        places = [h * block_rows + first for h in range(heads)]
        scores = []
        for h in range(heads):
            queries = q_ref[first : first + rows, h * head_dim : (h + 1) * head_dim]
            gate_q = column_ref[h, first : first + rows, 0:1]
            gate_k = gate_row(gates_ref, h, heads, origin, block_rows)
            scores.append(score(queries, key_ref[...], gate_q, gate_k, origin))
        wide = (rows, head_dim)
        held_tops = [top_ref[place : place + rows] for place in places]
        tops = [
            jnp.maximum(top, jnp.broadcast_to(jnp.max(s, axis=1, keepdims=True), wide))
            for top, s in zip(held_tops, scores)
        ]
        fades = [jnp.exp2(held_top - top) for held_top, top in zip(held_tops, tops)]
        weights = [faded(s, top) for s, top in zip(scores, tops)]
        dens = [
            den_ref[place : place + rows] * fade
            + jnp.broadcast_to(jnp.sum(weight, axis=1, keepdims=True), wide)
            for place, fade, weight in zip(places, fades, weights)
        ]
        sums = [
            jnp.dot(weight.astype(bf16), value_ref[...], preferred_element_type=f32)
            for weight in weights
        ]
        for h, place in enumerate(places):
            put(h, (acc_ref[place : place + rows] * fades[h] + sums[h]) / dens[h])

    out = jnp.dot(row_ref[...], weight_ref[...], preferred_element_type=f32)
    out_ref[...] = out.astype(bf16)


def pair_sum_kernel(keep_ref, got_ref, *outs):
    step = outs[0].shape[0]
    for i, out in enumerate(outs):
        rows = slice(i * step, (i + 1) * step)
        total = keep_ref[rows].astype(f32) + got_ref[rows].astype(f32)
        out[...] = total.astype(out.dtype)


def final_kernel(*refs):
    total = refs[0][...].astype(f32)
    for ref in refs[1:-1]:
        total = total + ref[...].astype(f32)
    refs[-1][...] = total.astype(bf16)


def layer(
    tokens,
    norm_gain,
    w_query,
    w_key,
    w_value,
    w_conv_value,
    w_conv_pre,
    w_conv_post,
    conv_taps,
    log_gate_cache,
    w_out_conv,
    w_out_attn,
):
    n_sp, n_fs, n_tp = lax.axis_size("sp"), lax.axis_size("fs"), lax.axis_size("tp")
    step, width = tokens.shape
    lane_rows = n_fs * step
    block_rows = n_tp * lane_rows
    channels = w_conv_post.shape[1]
    head_dim = w_key.shape[1]
    heads = w_query.shape[1] // head_dim

    def swapped(x):
        return lax.ppermute(x, "tp", [(0, 1), (1, 0)])

    def crossed(x, k):
        return lax.ppermute(x, "fs", [(i, i ^ k) for i in range(n_fs)])

    def raised(x, shift):
        route = [(i, (i + shift) % n_sp) for i in range(n_sp) if i + shift < n_sp or RING[shift]]
        return lax.ppermute(x, "sp", route)

    def call(kernel, out_shape, scratch, mib, *operands, in_specs=None, work=0):
        extra = {} if in_specs is None else {"in_specs": in_specs}
        if work:
            extra["cost_estimate"] = pl.CostEstimate(
                flops=work, transcendentals=0, bytes_accessed=0
            )
        return pl.pallas_call(
            kernel,
            out_shape=out_shape,
            scratch_shapes=scratch,
            compiler_params=kernel_params(mib),
            **extra,
        )(*operands)

    mask = call(mask_kernel, shape_of(block_rows, block_rows, f32), [], 4, work=MASK_WORK)
    normed = call(
        norm_kernel,
        shape_of(step, width),
        [],
        4,
        tokens,
        norm_gain.reshape(1, width),
        work=NORM_WORK,
    )
    w_post, w_pre, w_conv = w_conv_post, w_conv_pre, w_conv_value
    gates, taps = log_gate_cache, conv_taps
    own = [normed] + [crossed(normed, k) for k in range(1, n_fs)]
    other = [swapped(x) for x in own]
    pair = call(
        functools.partial(pair_kernel, n_fs),
        shape_of(lane_rows, 2 * head_dim),
        [pltpu.VMEM((lane_rows, width), bf16)],
        8,
        *own,
        w_key,
        w_value,
        work=SMALL_WORK,
    )
    halves = [pair, swapped(pair)]
    for shift in range(2, n_sp):
        piece = raised(pair, shift)
        halves += [piece, swapped(piece)]
    queries, post, mixed, rise = call(
        functools.partial(project_kernel, n_fs),
        (
            shape_of(block_rows, heads * head_dim),
            shape_of(block_rows, channels),
            shape_of(block_rows, channels),
            shape_of(lane_rows + EDGE, 2 * head_dim),
        ),
        [],
        16,
        *own,
        *other,
        w_query,
        w_post,
        w_pre,
        w_conv,
        pair,
        work=SMALL_WORK,
    )
    near = raised(rise, 1)
    far = swapped(near)
    held_shapes = (shape_of(heads * block_rows, head_dim, f32),) * 3
    *held, column = call(
        early_kernel,
        (*held_shapes, jax.ShapeDtypeStruct((heads, block_rows, 8), f32)),
        [pltpu.VMEM((block_rows, head_dim), bf16)] * 2 + [pltpu.VMEM((block_rows, 8), f32)],
        16,
        queries,
        gates,
        mask,
        *halves[:2],
        work=SMALL_WORK,
    )
    held = call(
        later_kernel,
        held_shapes,
        [pltpu.VMEM(((n_sp - 2) * block_rows, head_dim), bf16)] * 2,
        16,
        queries,
        gates,
        column,
        *held,
        *halves[2:],
        work=SMALL_WORK,
    )
    conv_out = call(
        functools.partial(conv_kernel, n_fs),
        shape_of(block_rows, channels),
        [pltpu.VMEM((block_rows + EDGE, channels), f32), pltpu.VMEM((block_rows, channels), f32)],
        4,
        post,
        mixed,
        near,
        taps,
        work=SMALL_WORK,
    )
    w_out = call(
        stack_kernel,
        shape_of(w_out_conv.shape[0] + w_out_attn.shape[0], width),
        [],
        8,
        w_out_conv,
        w_out_attn,
    )

    def mixed_rows(first):
        return call(
            functools.partial(mixer_kernel, first),
            shape_of(lane_rows, width),
            [pltpu.VMEM((block_rows, head_dim), bf16)] * 2
            + [pltpu.VMEM((lane_rows, channels + heads * head_dim), bf16)],
            16,
            queries,
            conv_out,
            gates,
            column,
            *held,
            near,
            far,
            w_out,
            work=SMALL_WORK,
        )

    send = mixed_rows(0)
    got = swapped(send)
    keep = mixed_rows(lane_rows)
    parts = range(n_fs - 1, -1, -1)
    pieces = call(
        pair_sum_kernel,
        tuple(shape_of(step, width, bf16 if k else f32) for k in parts),
        [],
        8,
        keep,
        got,
    )
    sums = [crossed(piece, k) if k else piece for k, piece in zip(parts, pieces)]
    return call(final_kernel, shape_of(step, width), [], 4, *sums)


def passed_along(block, axis, distance):
    devices = range(lax.axis_size(axis))
    route = [(i - distance, i) for i in devices if i - distance in devices]
    return lax.ppermute(block, axis, route)


def shards(
    tokens,
    norm_gain,
    w_query,
    w_key,
    w_value,
    w_conv_value,
    w_conv_pre,
    w_conv_post,
    conv_taps,
    log_gate_cache,
    w_out_conv,
    w_out_attn,
):
    float_rows = tokens.astype(jnp.float32)
    scaled = float_rows * lax.rsqrt(
        jnp.mean(float_rows * float_rows, axis=1, keepdims=True) + epsilon
    )
    normed_own = (scaled * norm_gain).astype(jnp.bfloat16)
    normed = lax.all_gather(normed_own, ("fs", "tp"), axis=0, tiled=True)
    block_rows = normed.shape[0]
    channels = w_conv_post.shape[1]
    head_dim = w_key.shape[1]
    local_heads = w_query.shape[1] // head_dim
    group = lax.axis_index(("fs", "tp"))
    local_weight = jnp.concatenate([w_conv_post, w_conv_pre, w_conv_value, w_query], axis=1)
    projected = jnp.dot(normed, local_weight, preferred_element_type=jnp.float32).astype(
        jnp.bfloat16
    )
    post_gate = projected[:, :channels]
    pre_gate = projected[:, channels : 2 * channels]
    conv_value = projected[:, 2 * channels : 3 * channels]
    queries = projected[:, 3 * channels :].reshape(block_rows, local_heads, head_dim)
    mixed_in = (pre_gate.astype(jnp.float32) * conv_value.astype(jnp.float32)).astype(jnp.bfloat16)
    kernel = conv_taps.shape[0]
    carried = passed_along(mixed_in[block_rows - (kernel - 1) :], "sp", 1)
    extended = jnp.concatenate([carried, mixed_in], axis=0).astype(jnp.float32)
    tap_weights = lax.dynamic_slice_in_dim(conv_taps, group * channels, channels, 1).astype(
        jnp.float32
    )
    conv_sum = tap_weights[0] * extended[0:block_rows]
    for offset in range(1, kernel):
        conv_sum = conv_sum + tap_weights[offset] * extended[offset : offset + block_rows]
    conv_out = (post_gate.astype(jnp.float32) * conv_sum).astype(jnp.bfloat16)
    core_index = lax.axis_index("tp")
    half_rows = block_rows // 2
    own_rows = lax.dynamic_slice_in_dim(normed, core_index * half_rows, half_rows, 0)
    pair_weight = jnp.concatenate([w_key, w_value], axis=1)
    pair_rows = jnp.dot(own_rows, pair_weight, preferred_element_type=jnp.float32).astype(
        jnp.bfloat16
    )
    key_half = pair_rows[:, :head_dim]
    value_half = pair_rows[:, head_dim:]
    head_gates = lax.dynamic_slice_in_dim(log_gate_cache, group * local_heads, local_heads, 0)
    anchor = lax.axis_index("sp") * block_rows
    gate_query = lax.dynamic_slice_in_dim(head_gates, anchor, block_rows, 1).T
    sequence_places = anchor + lax.iota(jnp.int32, block_rows)
    score_scale = head_dim ** (-0.5)

    def absorb(carried_state, key_block, value_block, sub_start):
        running_max, running_sum, weighted = carried_state
        sub_width = key_block.shape[0]
        scores = (
            jnp.einsum("qhd,kd->qhk", queries, key_block, preferred_element_type=jnp.float32)
            * score_scale
        )
        gate_keys = lax.dynamic_slice_in_dim(head_gates, sub_start, sub_width, 1)
        scores = scores + gate_query[:, :, None] - gate_keys[None, :, :]
        key_positions = sub_start + lax.iota(jnp.int32, sub_width)
        scores = jnp.where(
            sequence_places[:, None, None] >= key_positions[None, None, :], scores, masked_score
        )
        new_max = jnp.maximum(running_max, jnp.max(scores, axis=2))
        rescale = jnp.exp(running_max - new_max)
        weights = jnp.exp(scores - new_max[:, :, None])
        running_sum = running_sum * rescale + jnp.sum(weights, axis=2)
        weighted = weighted * rescale[:, :, None] + jnp.einsum(
            "qhk,kd->qhd",
            weights.astype(jnp.bfloat16),
            value_block,
            preferred_element_type=jnp.float32,
        )
        return (new_max, running_sum, weighted)

    initial = (
        jnp.full((block_rows, local_heads), masked_score, jnp.float32),
        jnp.zeros((block_rows, local_heads), jnp.float32),
        jnp.zeros((block_rows, local_heads, head_dim), jnp.float32),
    )
    key_piece = lax.all_gather(key_half, ("sp", "tp"), axis=0, tiled=True)
    value_piece = lax.all_gather(value_half, ("sp", "tp"), axis=0, tiled=True)
    key_count = key_piece.shape[0]
    sub_width = 512

    def sweep_keys(current):

        def absorb_step(running, step_index):
            sub_start = step_index * sub_width
            key_block = lax.dynamic_slice_in_dim(key_piece, sub_start, sub_width, 0)
            value_block = lax.dynamic_slice_in_dim(value_piece, sub_start, sub_width, 0)
            return (absorb(running, key_block, value_block, sub_start), None)

        result, _ = lax.scan(
            absorb_step, current, jnp.arange(key_count // sub_width, dtype=jnp.int32)
        )
        return result

    def keep_state(current):
        return current

    _, running_sum, weighted = lax.cond(
        jnp.int32(0) <= anchor + block_rows - 1, sweep_keys, keep_state, initial
    )
    attn_out = (
        (weighted / running_sum[:, :, None])
        .astype(jnp.bfloat16)
        .reshape(block_rows, local_heads * head_dim)
    )
    return lax.psum_scatter(
        (
            jnp.dot(conv_out, w_out_conv, preferred_element_type=jnp.float32)
            + jnp.dot(attn_out, w_out_attn, preferred_element_type=jnp.float32)
        ).astype(jnp.bfloat16),
        ("fs", "tp"),
        scatter_dimension=0,
        tiled=True,
    )


def solution(mesh):
    few = mesh.shape["sp"] == 4
    placed = (
        P(("sp", "fs", "tp"), None),
        P(),
        P(None, ("fs", "tp")),
        P(None, "fs"),
        P(None, "fs"),
        P(None, ("fs", "tp")),
        P(None, ("fs", "tp")),
        P(None, ("fs", "tp")),
        P(),
        P(),
        P(("fs", "tp"), None),
        P(("fs", "tp"), None),
    )
    return jax.shard_map(
        layer if few else shards,
        mesh=mesh,
        in_specs=placed,
        out_specs=P(("sp", "fs", "tp"), None),
        check_vma=False,
    )
```

```python
import functools
import math
import jax
import jax.numpy as jnp
from jax import lax
from jax.experimental import pallas as pl
from jax.experimental.pallas import tpu as pltpu
from jax.sharding import PartitionSpec as P

epsilon = 1e-06
masked_score = -1e30
log2e = math.log2(math.e)
f32 = jnp.float32
bf16 = jnp.bfloat16
EDGE = 16
RING = (False, False, True, True)
NORM_WORK = 20000000000
MASK_WORK = 2000000000
SMALL_WORK = 2000000000


def kernel_params(mib):
    return pltpu.CompilerParams(vmem_limit_bytes=mib * 1024 * 1024)


def shape_of(rows, cols, dtype=bf16):
    return jax.ShapeDtypeStruct((rows, cols), dtype)


def mask_kernel(out_ref):
    query_place = lax.broadcasted_iota(jnp.int32, out_ref.shape, 0)
    key_place = lax.broadcasted_iota(jnp.int32, out_ref.shape, 1)
    out_ref[...] = jnp.where(query_place >= key_place, 0.0, masked_score)


def norm_kernel(tokens_ref, gain_ref, out_ref):
    rows = tokens_ref[...].astype(f32)
    scale = lax.rsqrt(jnp.mean(rows * rows, axis=1, keepdims=True) + epsilon)
    out_ref[...] = (rows * scale * gain_ref[...]).astype(bf16)


def pair_kernel(n_fs, *refs):
    chunks, (w_key, w_value, out_ref, rows_ref) = refs[:n_fs], refs[n_fs:]
    step = chunks[0].shape[0]
    f = lax.axis_index("fs")
    for k in range(n_fs):
        rows_ref[pl.ds(pl.multiple_of((f ^ k) * step, step), step)] = chunks[k][...]
    weight = jnp.concatenate([w_key[...], w_value[...]], axis=1)
    out_ref[...] = jnp.dot(rows_ref[...], weight, preferred_element_type=f32).astype(bf16)


def place_pairs(pieces, key_ref, value_ref):
    head_dim = key_ref.shape[1]
    t = lax.axis_index("tp")
    n_fs = lax.axis_size("fs")
    step = key_ref.shape[0] // (2 * n_fs * len(pieces))
    for k, (near, far) in enumerate(pieces):
        for lane, piece in ((t, near), (1 - t, far)):
            for g in range(n_fs):
                place = (k * n_fs + g) * 2 * step + lane * step
                place = pl.ds(pl.multiple_of(place, step), step)
                key_ref[place] = piece[g * step : (g + 1) * step, :head_dim]
                value_ref[place] = piece[g * step : (g + 1) * step, head_dim:]


def gate_row(gates_ref, h, heads, origin, block_rows):
    group = lax.axis_index("fs") * lax.axis_size("tp") + lax.axis_index("tp")
    place = pl.multiple_of(jnp.maximum(origin, 0) * block_rows, block_rows)
    return gates_ref[pl.ds(group * heads + h, 1), pl.ds(place, block_rows)] * log2e


def score(queries, keys, gate_q, gate_k, origin):
    scale = queries.shape[1] ** (-0.5) * log2e
    s = lax.dot_general(
        queries, keys, (((1,), (1,)), ((), ())), preferred_element_type=f32
    )
    return s * scale + gate_q - jnp.where(origin >= 0, gate_k, -masked_score)


def faded(s, top):
    return jnp.exp2(s - jnp.concatenate([top] * (s.shape[1] // top.shape[1]), axis=1))


def fold_blocks(q_ref, gates_ref, column_ref, blocks, masks, held, outs):
    acc_ref, top_ref, den_ref = outs
    block_rows = q_ref.shape[0]
    head_dim = acc_ref.shape[1]
    heads = q_ref.shape[1] // head_dim
    tile = block_rows // 2
    tiles = [(h, i) for h in range(heads) for i in range(0, block_rows, tile)]
    places = [slice(h * block_rows + i, h * block_rows + i + tile) for h, i in tiles]
    scores = []
    for h, i in tiles:
        queries = q_ref[i : i + tile, h * head_dim : (h + 1) * head_dim]
        gate_q = column_ref[h, i : i + tile, 0:1]
        row = []
        for keys, values, origin in blocks:
            gate_k = gate_row(gates_ref, h, heads, origin, block_rows)
            s = score(queries, keys, gate_q, gate_k, origin)
            row.append(s + masks[i // tile] if masks else s)
        scores.append(row)
    wide = (tile, head_dim)
    tops = [
        jnp.broadcast_to(
            jnp.max(functools.reduce(jnp.maximum, row), axis=1, keepdims=True), wide
        )
        for row in scores
    ]
    if held:
        held_tops = [held[1][place] for place in places]
        tops = [jnp.maximum(top, held_top) for top, held_top in zip(tops, held_tops)]
        fades = [jnp.exp2(held_top - top) for top, held_top in zip(tops, held_tops)]
    weights = [[faded(s, top) for s in row] for row, top in zip(scores, tops)]
    dens = [
        jnp.broadcast_to(jnp.sum(sum(row), axis=1, keepdims=True), wide) for row in weights
    ]
    for n, place in enumerate(places):
        total = sum(
            jnp.dot(weight.astype(bf16), values, preferred_element_type=f32)
            for weight, (keys, values, origin) in zip(weights[n], blocks)
        )
        den = dens[n]
        if held:
            total = total + held[0][place] * fades[n]
            den = den + held[2][place] * fades[n]
        acc_ref[place] = total
        top_ref[place] = tops[n]
        den_ref[place] = den


def early_kernel(*refs):
    q_ref, gates_ref, mask_ref, near_ref, far_ref = refs[:5]
    outs, (column_ref, key_ref, value_ref, natural_ref) = refs[5:8], refs[8:]
    place_pairs(((near_ref, far_ref),), key_ref, value_ref)
    z = lax.axis_index("sp")
    block_rows = q_ref.shape[0]
    heads = column_ref.shape[0]
    n_fs = lax.axis_size("fs")
    step = block_rows // (2 * n_fs)
    places = row_places(n_fs, step)
    for h in range(heads):
        row = gate_row(gates_ref, h, heads, z, block_rows)
        natural_ref[...] = jnp.broadcast_to(row, (8, block_rows)).T
        for i, place in enumerate(places):
            column_ref[h, i * step : (i + 1) * step] = natural_ref[pl.ds(place, step)]
    masks = []
    for i in range(0, 2 * n_fs, n_fs):
        piece = [mask_ref[pl.ds(place, step)] for place in places[i : i + n_fs]]
        masks.append(jnp.concatenate(piece, axis=0))
    blocks = [(key_ref[...], value_ref[...], z)]
    fold_blocks(q_ref, gates_ref, column_ref, blocks, masks, None, outs)


def later_kernel(*refs):
    q_ref, gates_ref, column_ref = refs[:3]
    held, outs, (key_ref, value_ref) = refs[3:6], refs[-5:-2], refs[-2:]
    pieces = tuple(zip(refs[6:-5:2], refs[7:-5:2]))
    z = lax.axis_index("sp")
    block_rows = q_ref.shape[0]

    def keep():
        for source, out in zip(held, outs):
            out[...] = source[...]

    def fold(count):
        rows = slice(0, count * block_rows)
        place_pairs(pieces[:count], key_ref.at[rows], value_ref.at[rows])
        blocks = []
        for k in range(count):
            rows = slice(k * block_rows, (k + 1) * block_rows)
            blocks.append((key_ref[rows], value_ref[rows], z - 2 - k))
        fold_blocks(q_ref, gates_ref, column_ref, blocks, None, held, outs)

    pl.when(z < 2)(keep)
    for count in range(1, len(pieces) + 1):
        pl.when(z - 1 == count)(functools.partial(fold, count))


def row_places(n_fs, step):
    f = lax.axis_index("fs")
    t = lax.axis_index("tp")
    return [
        pl.multiple_of((f ^ k) * 2 * step + lane * step, step)
        for lane in (1 - t, t)
        for k in range(n_fs - 1, -1, -1)
    ]


def project_kernel(n_fs, *refs):
    own, other = refs[:n_fs], refs[n_fs : 2 * n_fs]
    w_query, w_post, w_pre, w_conv, pair_ref = refs[2 * n_fs : 2 * n_fs + 5]
    q_ref, post_ref, mixed_ref, rise_ref = refs[2 * n_fs + 5 :]
    step = own[0].shape[0]
    rows = jnp.concatenate([ref[...] for ref in (*other[::-1], *own[::-1])], axis=0)
    weight = jnp.concatenate([w_pre[...], w_conv[...]], axis=1)
    gated = jnp.dot(rows, weight, preferred_element_type=f32).astype(bf16).astype(f32)
    channels = w_pre.shape[1]
    mixed = (gated[:, :channels] * gated[:, channels:]).astype(bf16)
    for i, place in enumerate(row_places(n_fs, step)):
        mixed_ref[pl.ds(place, step)] = mixed[i * step : (i + 1) * step]
    lane_rows = pair_ref.shape[0]
    rise_ref[:lane_rows] = pair_ref[...]
    last = mixed_ref[mixed_ref.shape[0] - EDGE :]
    rise_ref[lane_rows:] = jnp.concatenate([last] * (rise_ref.shape[1] // channels), axis=1)
    q_ref[...] = jnp.dot(rows, w_query[...], preferred_element_type=f32).astype(bf16)
    post_ref[...] = jnp.dot(rows, w_post[...], preferred_element_type=f32).astype(bf16)


def stack_kernel(top_ref, low_ref, out_ref):
    out_ref[: top_ref.shape[0]] = top_ref[...]
    out_ref[top_ref.shape[0] :] = low_ref[...]


def conv_kernel(n_fs, post_ref, mixed_ref, risen_ref, taps_ref, out_ref, extended_ref, sum_ref):
    block_rows, channels = mixed_ref.shape
    group = lax.axis_index("fs") * lax.axis_size("tp") + lax.axis_index("tp")
    lanes = pl.ds(pl.multiple_of(group * channels, channels), channels)
    taps = taps_ref.shape[0]
    halo = risen_ref[risen_ref.shape[0] - EDGE :, :channels].astype(f32)
    extended_ref[0:EDGE] = jnp.where(lax.axis_index("sp") > 0, halo, 0.0)
    extended_ref[EDGE:] = mixed_ref[...].astype(f32)
    tap_rows = taps_ref[:, lanes].astype(f32)
    first = EDGE - (taps - 1)
    conv_sum = tap_rows[0:1] * extended_ref[first : first + block_rows]
    for i in range(1, taps):
        conv_sum = conv_sum + tap_rows[i : i + 1] * extended_ref[first + i : first + i + block_rows]
    sum_ref[...] = conv_sum
    step = block_rows // (2 * n_fs)
    for i, place in enumerate(row_places(n_fs, step)):
        rows = slice(i * step, (i + 1) * step)
        out_ref[rows] = (post_ref[rows].astype(f32) * sum_ref[pl.ds(place, step)]).astype(bf16)


def mixer_kernel(first, *refs):
    q_ref, conv_ref, gates_ref, column_ref, acc_ref, top_ref, den_ref = refs[:7]
    near_ref, far_ref, weight_ref = refs[7:10]
    outs, (key_ref, value_ref, row_ref) = refs[10:-3], refs[-3:]
    block_rows = q_ref.shape[0]
    head_dim = key_ref.shape[1]
    channels = conv_ref.shape[1]
    heads = q_ref.shape[1] // head_dim
    rows = sum(out_ref.shape[0] for out_ref in outs)
    origin = lax.axis_index("sp") - 1
    row_ref[:, :channels] = conv_ref[first : first + rows]

    def put(h, value):
        place = channels + h * head_dim
        row_ref[:, place : place + head_dim] = value.astype(bf16)

    @pl.when(origin < 0)
    def alone():
        for h in range(heads):
            place = h * block_rows + first
            put(h, acc_ref[place : place + rows] / den_ref[place : place + rows])

    @pl.when(origin >= 0)
    def joined():
        place_pairs(((near_ref, far_ref),), key_ref, value_ref)
        places = [h * block_rows + first for h in range(heads)]
        scores = []
        for h in range(heads):
            queries = q_ref[first : first + rows, h * head_dim : (h + 1) * head_dim]
            gate_q = column_ref[h, first : first + rows, 0:1]
            gate_k = gate_row(gates_ref, h, heads, origin, block_rows)
            scores.append(score(queries, key_ref[...], gate_q, gate_k, origin))
        wide = (rows, head_dim)
        held_tops = [top_ref[place : place + rows] for place in places]
        tops = [
            jnp.maximum(top, jnp.broadcast_to(jnp.max(s, axis=1, keepdims=True), wide))
            for top, s in zip(held_tops, scores)
        ]
        fades = [jnp.exp2(held_top - top) for held_top, top in zip(held_tops, tops)]
        weights = [faded(s, top) for s, top in zip(scores, tops)]
        dens = [
            den_ref[place : place + rows] * fade
            + jnp.broadcast_to(jnp.sum(weight, axis=1, keepdims=True), wide)
            for place, fade, weight in zip(places, fades, weights)
        ]
        sums = [
            jnp.dot(weight.astype(bf16), value_ref[...], preferred_element_type=f32)
            for weight in weights
        ]
        for h, place in enumerate(places):
            put(h, (acc_ref[place : place + rows] * fades[h] + sums[h]) / dens[h])

    out = jnp.dot(row_ref[...], weight_ref[...], preferred_element_type=f32).astype(bf16)
    start = 0
    for out_ref in outs:
        out_ref[...] = out[start : start + out_ref.shape[0]]
        start += out_ref.shape[0]


def pair_sum_kernel(keep_ref, got_ref, *outs):
    step = outs[0].shape[0]
    for i, out in enumerate(outs):
        rows = slice(i * step, (i + 1) * step)
        total = keep_ref[rows].astype(f32) + got_ref[rows].astype(f32)
        out[...] = total.astype(out.dtype)


def final_kernel(*refs):
    total = refs[0][...].astype(f32)
    for ref in refs[1:-1]:
        total = total + ref[...].astype(f32)
    refs[-1][...] = total.astype(bf16)


def layer(
    tokens,
    norm_gain,
    w_query,
    w_key,
    w_value,
    w_conv_value,
    w_conv_pre,
    w_conv_post,
    conv_taps,
    log_gate_cache,
    w_out_conv,
    w_out_attn,
):
    n_sp, n_fs, n_tp = lax.axis_size("sp"), lax.axis_size("fs"), lax.axis_size("tp")
    step, width = tokens.shape
    lane_rows = n_fs * step
    block_rows = n_tp * lane_rows
    channels = w_conv_post.shape[1]
    head_dim = w_key.shape[1]
    heads = w_query.shape[1] // head_dim

    def swapped(x):
        return lax.ppermute(x, "tp", [(0, 1), (1, 0)])

    def crossed(x, k):
        return lax.ppermute(x, "fs", [(i, i ^ k) for i in range(n_fs)])

    def raised(x, shift):
        route = [(i, (i + shift) % n_sp) for i in range(n_sp) if i + shift < n_sp or RING[shift]]
        return lax.ppermute(x, "sp", route)

    def call(kernel, out_shape, scratch, mib, *operands, in_specs=None, work=0):
        extra = {} if in_specs is None else {"in_specs": in_specs}
        if work:
            extra["cost_estimate"] = pl.CostEstimate(
                flops=work, transcendentals=0, bytes_accessed=0
            )
        return pl.pallas_call(
            kernel,
            out_shape=out_shape,
            scratch_shapes=scratch,
            compiler_params=kernel_params(mib),
            **extra,
        )(*operands)

    mask = call(mask_kernel, shape_of(block_rows, block_rows, f32), [], 4, work=MASK_WORK)
    normed = call(
        norm_kernel,
        shape_of(step, width),
        [],
        4,
        tokens,
        norm_gain.reshape(1, width),
        work=NORM_WORK,
    )
    w_post, w_pre, w_conv = w_conv_post, w_conv_pre, w_conv_value
    gates, taps = log_gate_cache, conv_taps
    own = [normed] + [crossed(normed, k) for k in range(1, n_fs)]
    other = [swapped(x) for x in own]
    pair = call(
        functools.partial(pair_kernel, n_fs),
        shape_of(lane_rows, 2 * head_dim),
        [pltpu.VMEM((lane_rows, width), bf16)],
        8,
        *own,
        w_key,
        w_value,
        work=SMALL_WORK,
    )
    halves = [pair, swapped(pair)]
    for shift in range(2, n_sp):
        piece = raised(pair, shift)
        halves += [piece, swapped(piece)]
    queries, post, mixed, rise = call(
        functools.partial(project_kernel, n_fs),
        (
            shape_of(block_rows, heads * head_dim),
            shape_of(block_rows, channels),
            shape_of(block_rows, channels),
            shape_of(lane_rows + EDGE, 2 * head_dim),
        ),
        [],
        16,
        *own,
        *other,
        w_query,
        w_post,
        w_pre,
        w_conv,
        pair,
        work=SMALL_WORK,
    )
    near = raised(rise, 1)
    far = swapped(near)
    held_shapes = (shape_of(heads * block_rows, head_dim, f32),) * 3
    *held, column = call(
        early_kernel,
        (*held_shapes, jax.ShapeDtypeStruct((heads, block_rows, 8), f32)),
        [pltpu.VMEM((block_rows, head_dim), bf16)] * 2 + [pltpu.VMEM((block_rows, 8), f32)],
        16,
        queries,
        gates,
        mask,
        *halves[:2],
        work=SMALL_WORK,
    )
    held = call(
        later_kernel,
        held_shapes,
        [pltpu.VMEM(((n_sp - 2) * block_rows, head_dim), bf16)] * 2,
        16,
        queries,
        gates,
        column,
        *held,
        *halves[2:],
        work=SMALL_WORK,
    )
    conv_out = call(
        functools.partial(conv_kernel, n_fs),
        shape_of(block_rows, channels),
        [pltpu.VMEM((block_rows + EDGE, channels), f32), pltpu.VMEM((block_rows, channels), f32)],
        4,
        post,
        mixed,
        near,
        taps,
        work=SMALL_WORK,
    )
    w_out = call(
        stack_kernel,
        shape_of(w_out_conv.shape[0] + w_out_attn.shape[0], width),
        [],
        8,
        w_out_conv,
        w_out_attn,
    )

    def mixed_rows(first):
        return call(
            functools.partial(mixer_kernel, first),
            tuple(shape_of(count * step, width) for count in (1, n_fs - 1)),
            [pltpu.VMEM((block_rows, head_dim), bf16)] * 2
            + [pltpu.VMEM((lane_rows, channels + heads * head_dim), bf16)],
            16,
            queries,
            conv_out,
            gates,
            column,
            *held,
            near,
            far,
            w_out,
            work=SMALL_WORK,
        )

    counts = (1, n_fs - 1)
    sends = mixed_rows(0)
    gots = [swapped(send) for send in sends]
    keeps = mixed_rows(lane_rows)
    parts = list(range(n_fs - 1, -1, -1))
    sums = []
    for count, keep, got in zip(counts, keeps, gots):
        group, parts = parts[:count], parts[count:]
        pieces = call(
            pair_sum_kernel,
            tuple(shape_of(step, width, bf16 if k else f32) for k in group),
            [],
            8,
            keep,
            got,
        )
        sums += [crossed(piece, k) if k else piece for k, piece in zip(group, pieces)]
    return call(final_kernel, shape_of(step, width), [], 4, *sums)


def passed_along(block, axis, distance):
    devices = range(lax.axis_size(axis))
    route = [(i - distance, i) for i in devices if i - distance in devices]
    return lax.ppermute(block, axis, route)


def shards(
    tokens,
    norm_gain,
    w_query,
    w_key,
    w_value,
    w_conv_value,
    w_conv_pre,
    w_conv_post,
    conv_taps,
    log_gate_cache,
    w_out_conv,
    w_out_attn,
):
    float_rows = tokens.astype(jnp.float32)
    scaled = float_rows * lax.rsqrt(
        jnp.mean(float_rows * float_rows, axis=1, keepdims=True) + epsilon
    )
    normed_own = (scaled * norm_gain).astype(jnp.bfloat16)
    normed = lax.all_gather(normed_own, ("fs", "tp"), axis=0, tiled=True)
    block_rows = normed.shape[0]
    channels = w_conv_post.shape[1]
    head_dim = w_key.shape[1]
    local_heads = w_query.shape[1] // head_dim
    group = lax.axis_index(("fs", "tp"))
    local_weight = jnp.concatenate([w_conv_post, w_conv_pre, w_conv_value, w_query], axis=1)
    projected = jnp.dot(normed, local_weight, preferred_element_type=jnp.float32).astype(
        jnp.bfloat16
    )
    post_gate = projected[:, :channels]
    pre_gate = projected[:, channels : 2 * channels]
    conv_value = projected[:, 2 * channels : 3 * channels]
    queries = projected[:, 3 * channels :].reshape(block_rows, local_heads, head_dim)
    mixed_in = (pre_gate.astype(jnp.float32) * conv_value.astype(jnp.float32)).astype(jnp.bfloat16)
    kernel = conv_taps.shape[0]
    carried = passed_along(mixed_in[block_rows - (kernel - 1) :], "sp", 1)
    extended = jnp.concatenate([carried, mixed_in], axis=0).astype(jnp.float32)
    tap_weights = lax.dynamic_slice_in_dim(conv_taps, group * channels, channels, 1).astype(
        jnp.float32
    )
    conv_sum = tap_weights[0] * extended[0:block_rows]
    for offset in range(1, kernel):
        conv_sum = conv_sum + tap_weights[offset] * extended[offset : offset + block_rows]
    conv_out = (post_gate.astype(jnp.float32) * conv_sum).astype(jnp.bfloat16)
    core_index = lax.axis_index("tp")
    half_rows = block_rows // 2
    own_rows = lax.dynamic_slice_in_dim(normed, core_index * half_rows, half_rows, 0)
    pair_weight = jnp.concatenate([w_key, w_value], axis=1)
    pair_rows = jnp.dot(own_rows, pair_weight, preferred_element_type=jnp.float32).astype(
        jnp.bfloat16
    )
    key_half = pair_rows[:, :head_dim]
    value_half = pair_rows[:, head_dim:]
    head_gates = lax.dynamic_slice_in_dim(log_gate_cache, group * local_heads, local_heads, 0)
    anchor = lax.axis_index("sp") * block_rows
    gate_query = lax.dynamic_slice_in_dim(head_gates, anchor, block_rows, 1).T
    sequence_places = anchor + lax.iota(jnp.int32, block_rows)
    score_scale = head_dim ** (-0.5)

    def absorb(carried_state, key_block, value_block, sub_start):
        running_max, running_sum, weighted = carried_state
        sub_width = key_block.shape[0]
        scores = (
            jnp.einsum("qhd,kd->qhk", queries, key_block, preferred_element_type=jnp.float32)
            * score_scale
        )
        gate_keys = lax.dynamic_slice_in_dim(head_gates, sub_start, sub_width, 1)
        scores = scores + gate_query[:, :, None] - gate_keys[None, :, :]
        key_positions = sub_start + lax.iota(jnp.int32, sub_width)
        scores = jnp.where(
            sequence_places[:, None, None] >= key_positions[None, None, :], scores, masked_score
        )
        new_max = jnp.maximum(running_max, jnp.max(scores, axis=2))
        rescale = jnp.exp(running_max - new_max)
        weights = jnp.exp(scores - new_max[:, :, None])
        running_sum = running_sum * rescale + jnp.sum(weights, axis=2)
        weighted = weighted * rescale[:, :, None] + jnp.einsum(
            "qhk,kd->qhd",
            weights.astype(jnp.bfloat16),
            value_block,
            preferred_element_type=jnp.float32,
        )
        return (new_max, running_sum, weighted)

    initial = (
        jnp.full((block_rows, local_heads), masked_score, jnp.float32),
        jnp.zeros((block_rows, local_heads), jnp.float32),
        jnp.zeros((block_rows, local_heads, head_dim), jnp.float32),
    )
    key_piece = lax.all_gather(key_half, ("sp", "tp"), axis=0, tiled=True)
    value_piece = lax.all_gather(value_half, ("sp", "tp"), axis=0, tiled=True)
    key_count = key_piece.shape[0]
    sub_width = 512

    def sweep_keys(current):

        def absorb_step(running, step_index):
            sub_start = step_index * sub_width
            key_block = lax.dynamic_slice_in_dim(key_piece, sub_start, sub_width, 0)
            value_block = lax.dynamic_slice_in_dim(value_piece, sub_start, sub_width, 0)
            return (absorb(running, key_block, value_block, sub_start), None)

        result, _ = lax.scan(
            absorb_step, current, jnp.arange(key_count // sub_width, dtype=jnp.int32)
        )
        return result

    def keep_state(current):
        return current

    _, running_sum, weighted = lax.cond(
        jnp.int32(0) <= anchor + block_rows - 1, sweep_keys, keep_state, initial
    )
    attn_out = (
        (weighted / running_sum[:, :, None])
        .astype(jnp.bfloat16)
        .reshape(block_rows, local_heads * head_dim)
    )
    return lax.psum_scatter(
        (
            jnp.dot(conv_out, w_out_conv, preferred_element_type=jnp.float32)
            + jnp.dot(attn_out, w_out_attn, preferred_element_type=jnp.float32)
        ).astype(jnp.bfloat16),
        ("fs", "tp"),
        scatter_dimension=0,
        tiled=True,
    )


def solution(mesh):
    few = mesh.shape["sp"] == 4
    placed = (
        P(("sp", "fs", "tp"), None),
        P(),
        P(None, ("fs", "tp")),
        P(None, "fs"),
        P(None, "fs"),
        P(None, ("fs", "tp")),
        P(None, ("fs", "tp")),
        P(None, ("fs", "tp")),
        P(),
        P(),
        P(("fs", "tp"), None),
        P(("fs", "tp"), None),
    )
    return jax.shard_map(
        layer if few else shards,
        mesh=mesh,
        in_specs=placed,
        out_specs=P(("sp", "fs", "tp"), None),
        check_vma=False,
    )
```

```python
import functools
import math
import jax
import jax.numpy as jnp
from jax import lax
from jax.experimental import pallas as pl
from jax.experimental.pallas import tpu as pltpu
from jax.sharding import PartitionSpec as P

epsilon = 1e-06
masked_score = -1e30
log2e = math.log2(math.e)
f32 = jnp.float32
bf16 = jnp.bfloat16
EDGE = 16
RING = (False, False, True, True)
NORM_WORK = 20000000000
MASK_WORK = 2000000000
SMALL_WORK = 2000000000


def kernel_params(mib):
    return pltpu.CompilerParams(vmem_limit_bytes=mib * 1024 * 1024)


def shape_of(rows, cols, dtype=bf16):
    return jax.ShapeDtypeStruct((rows, cols), dtype)


def mask_kernel(out_ref):
    query_place = lax.broadcasted_iota(jnp.int32, out_ref.shape, 0)
    key_place = lax.broadcasted_iota(jnp.int32, out_ref.shape, 1)
    out_ref[...] = jnp.where(query_place >= key_place, 0.0, masked_score)


def norm_kernel(tokens_ref, gain_ref, out_ref):
    rows = tokens_ref[...].astype(f32)
    scale = lax.rsqrt(jnp.mean(rows * rows, axis=1, keepdims=True) + epsilon)
    out_ref[...] = (rows * scale * gain_ref[...]).astype(bf16)


def pair_kernel(n_fs, *refs):
    chunks, (w_key, w_value, out_ref, rows_ref) = refs[:n_fs], refs[n_fs:]
    step = chunks[0].shape[0]
    f = lax.axis_index("fs")
    for k in range(n_fs):
        rows_ref[pl.ds(pl.multiple_of((f ^ k) * step, step), step)] = chunks[k][...]
    weight = jnp.concatenate([w_key[...], w_value[...]], axis=1)
    out_ref[...] = jnp.dot(rows_ref[...], weight, preferred_element_type=f32).astype(bf16)


def place_pairs(pieces, key_ref, value_ref):
    head_dim = key_ref.shape[1]
    t = lax.axis_index("tp")
    n_fs = lax.axis_size("fs")
    step = key_ref.shape[0] // (2 * n_fs * len(pieces))
    for k, (near, far) in enumerate(pieces):
        for lane, piece in ((t, near), (1 - t, far)):
            for g in range(n_fs):
                place = (k * n_fs + g) * 2 * step + lane * step
                place = pl.ds(pl.multiple_of(place, step), step)
                key_ref[place] = piece[g * step : (g + 1) * step, :head_dim]
                value_ref[place] = piece[g * step : (g + 1) * step, head_dim:]


def gate_row(gates_ref, h, heads, origin, block_rows):
    group = lax.axis_index("fs") * lax.axis_size("tp") + lax.axis_index("tp")
    place = pl.multiple_of(jnp.maximum(origin, 0) * block_rows, block_rows)
    return gates_ref[pl.ds(group * heads + h, 1), pl.ds(place, block_rows)] * log2e


def score(queries, keys, gate_q, gate_k, origin):
    scale = queries.shape[1] ** (-0.5) * log2e
    s = lax.dot_general(
        queries, keys, (((1,), (1,)), ((), ())), preferred_element_type=f32
    )
    return s * scale + gate_q - jnp.where(origin >= 0, gate_k, -masked_score)


def faded(s, top):
    return jnp.exp2(s - jnp.concatenate([top] * (s.shape[1] // top.shape[1]), axis=1))


def fold_blocks(q_ref, gates_ref, column_ref, blocks, masks, held, outs):
    acc_ref, top_ref, den_ref = outs
    block_rows = q_ref.shape[0]
    head_dim = acc_ref.shape[1]
    heads = q_ref.shape[1] // head_dim
    tile = block_rows // 2
    tiles = [(h, i) for h in range(heads) for i in range(0, block_rows, tile)]
    places = [slice(h * block_rows + i, h * block_rows + i + tile) for h, i in tiles]
    scores = []
    for h, i in tiles:
        queries = q_ref[i : i + tile, h * head_dim : (h + 1) * head_dim]
        gate_q = column_ref[h, i : i + tile, 0:1]
        row = []
        for keys, values, origin in blocks:
            gate_k = gate_row(gates_ref, h, heads, origin, block_rows)
            s = score(queries, keys, gate_q, gate_k, origin)
            row.append(s + masks[i // tile] if masks else s)
        scores.append(row)
    wide = (tile, head_dim)
    tops = [
        jnp.broadcast_to(
            jnp.max(functools.reduce(jnp.maximum, row), axis=1, keepdims=True), wide
        )
        for row in scores
    ]
    if held:
        held_tops = [held[1][place] for place in places]
        tops = [jnp.maximum(top, held_top) for top, held_top in zip(tops, held_tops)]
        fades = [jnp.exp2(held_top - top) for top, held_top in zip(tops, held_tops)]
    weights = [[faded(s, top) for s in row] for row, top in zip(scores, tops)]
    dens = [
        jnp.broadcast_to(jnp.sum(sum(row), axis=1, keepdims=True), wide) for row in weights
    ]
    for n, place in enumerate(places):
        total = sum(
            jnp.dot(weight.astype(bf16), values, preferred_element_type=f32)
            for weight, (keys, values, origin) in zip(weights[n], blocks)
        )
        den = dens[n]
        if held:
            total = total + held[0][place] * fades[n]
            den = den + held[2][place] * fades[n]
        acc_ref[place] = total
        top_ref[place] = tops[n]
        den_ref[place] = den


def early_kernel(*refs):
    q_ref, gates_ref, mask_ref, taps_ref, near_ref, far_ref = refs[:6]
    outs, (column_ref, tap_ref, key_ref, value_ref, natural_ref) = refs[6:9], refs[9:]
    group = lax.axis_index("fs") * lax.axis_size("tp") + lax.axis_index("tp")
    channels = tap_ref.shape[1]
    lanes = pl.ds(pl.multiple_of(group * channels, channels), channels)
    tap_ref[...] = taps_ref[:, lanes].astype(f32)
    place_pairs(((near_ref, far_ref),), key_ref, value_ref)
    z = lax.axis_index("sp")
    block_rows = q_ref.shape[0]
    heads = column_ref.shape[0]
    n_fs = lax.axis_size("fs")
    step = block_rows // (2 * n_fs)
    places = row_places(n_fs, step)
    for h in range(heads):
        row = gate_row(gates_ref, h, heads, z, block_rows)
        natural_ref[...] = jnp.broadcast_to(row, (8, block_rows)).T
        for i, place in enumerate(places):
            column_ref[h, i * step : (i + 1) * step] = natural_ref[pl.ds(place, step)]
    masks = []
    for i in range(0, 2 * n_fs, n_fs):
        piece = [mask_ref[pl.ds(place, step)] for place in places[i : i + n_fs]]
        masks.append(jnp.concatenate(piece, axis=0))
    blocks = [(key_ref[...], value_ref[...], z)]
    fold_blocks(q_ref, gates_ref, column_ref, blocks, masks, None, outs)


def later_kernel(*refs):
    q_ref, gates_ref, column_ref = refs[:3]
    held, outs, (key_ref, value_ref) = refs[3:6], refs[-5:-2], refs[-2:]
    pieces = tuple(zip(refs[6:-5:2], refs[7:-5:2]))
    z = lax.axis_index("sp")
    block_rows = q_ref.shape[0]

    def keep():
        for source, out in zip(held, outs):
            out[...] = source[...]

    def fold(count):
        rows = slice(0, count * block_rows)
        place_pairs(pieces[:count], key_ref.at[rows], value_ref.at[rows])
        blocks = []
        for k in range(count):
            rows = slice(k * block_rows, (k + 1) * block_rows)
            blocks.append((key_ref[rows], value_ref[rows], z - 2 - k))
        fold_blocks(q_ref, gates_ref, column_ref, blocks, None, held, outs)

    pl.when(z < 2)(keep)
    for count in range(1, len(pieces) + 1):
        pl.when(z - 1 == count)(functools.partial(fold, count))


def row_places(n_fs, step):
    f = lax.axis_index("fs")
    t = lax.axis_index("tp")
    return [
        pl.multiple_of((f ^ k) * 2 * step + lane * step, step)
        for lane in (1 - t, t)
        for k in range(n_fs - 1, -1, -1)
    ]


def gathered(own, other):
    return jnp.concatenate([ref[...] for ref in (*other[::-1], *own[::-1])], axis=0)


def gate_kernel(n_fs, *refs):
    own, other = refs[:n_fs], refs[n_fs : 2 * n_fs]
    w_pre, w_conv, pair_ref, mixed_ref, rise_ref = refs[2 * n_fs :]
    step = own[0].shape[0]
    rows = gathered(own, other)
    weight = jnp.concatenate([w_pre[...], w_conv[...]], axis=1)
    gated = jnp.dot(rows, weight, preferred_element_type=f32).astype(bf16).astype(f32)
    channels = w_pre.shape[1]
    mixed = (gated[:, :channels] * gated[:, channels:]).astype(bf16)
    for i, place in enumerate(row_places(n_fs, step)):
        mixed_ref[pl.ds(place, step)] = mixed[i * step : (i + 1) * step]
    lane_rows = pair_ref.shape[0]
    rise_ref[:lane_rows] = pair_ref[...]
    last = mixed_ref[mixed_ref.shape[0] - EDGE :]
    rise_ref[lane_rows:] = jnp.concatenate([last] * (rise_ref.shape[1] // channels), axis=1)


def query_kernel(n_fs, *refs):
    rows = gathered(refs[:n_fs], refs[n_fs : 2 * n_fs])
    w_query, w_post, q_ref, post_ref = refs[2 * n_fs :]
    q_ref[...] = jnp.dot(rows, w_query[...], preferred_element_type=f32).astype(bf16)
    post_ref[...] = jnp.dot(rows, w_post[...], preferred_element_type=f32).astype(bf16)


def stack_kernel(top_ref, low_ref, out_ref):
    out_ref[: top_ref.shape[0]] = top_ref[...]
    out_ref[top_ref.shape[0] :] = low_ref[...]


def conv_kernel(n_fs, post_ref, mixed_ref, risen_ref, taps_ref, out_ref, extended_ref, sum_ref):
    block_rows, channels = mixed_ref.shape
    taps = taps_ref.shape[0]
    halo = risen_ref[risen_ref.shape[0] - EDGE :, :channels].astype(f32)
    extended_ref[0:EDGE] = jnp.where(lax.axis_index("sp") > 0, halo, 0.0)
    extended_ref[EDGE:] = mixed_ref[...].astype(f32)
    tap_rows = taps_ref[...]
    first = EDGE - (taps - 1)
    conv_sum = tap_rows[0:1] * extended_ref[first : first + block_rows]
    for i in range(1, taps):
        conv_sum = conv_sum + tap_rows[i : i + 1] * extended_ref[first + i : first + i + block_rows]
    sum_ref[...] = conv_sum
    step = block_rows // (2 * n_fs)
    for i, place in enumerate(row_places(n_fs, step)):
        rows = slice(i * step, (i + 1) * step)
        out_ref[rows] = (post_ref[rows].astype(f32) * sum_ref[pl.ds(place, step)]).astype(bf16)


def mixer_kernel(first, *refs):
    q_ref, conv_ref, gates_ref, column_ref, acc_ref, top_ref, den_ref = refs[:7]
    near_ref, far_ref, weight_ref = refs[7:10]
    outs, (key_ref, value_ref, row_ref) = refs[10:-3], refs[-3:]
    block_rows = q_ref.shape[0]
    head_dim = key_ref.shape[1]
    channels = conv_ref.shape[1]
    heads = q_ref.shape[1] // head_dim
    rows = sum(out_ref.shape[0] for out_ref in outs)
    origin = lax.axis_index("sp") - 1
    row_ref[:, :channels] = conv_ref[first : first + rows]

    def put(h, value):
        place = channels + h * head_dim
        row_ref[:, place : place + head_dim] = value.astype(bf16)

    @pl.when(origin < 0)
    def alone():
        for h in range(heads):
            place = h * block_rows + first
            put(h, acc_ref[place : place + rows] / den_ref[place : place + rows])

    @pl.when(origin >= 0)
    def joined():
        place_pairs(((near_ref, far_ref),), key_ref, value_ref)
        places = [h * block_rows + first for h in range(heads)]
        scores = []
        for h in range(heads):
            queries = q_ref[first : first + rows, h * head_dim : (h + 1) * head_dim]
            gate_q = column_ref[h, first : first + rows, 0:1]
            gate_k = gate_row(gates_ref, h, heads, origin, block_rows)
            scores.append(score(queries, key_ref[...], gate_q, gate_k, origin))
        wide = (rows, head_dim)
        held_tops = [top_ref[place : place + rows] for place in places]
        tops = [
            jnp.maximum(top, jnp.broadcast_to(jnp.max(s, axis=1, keepdims=True), wide))
            for top, s in zip(held_tops, scores)
        ]
        fades = [jnp.exp2(held_top - top) for held_top, top in zip(held_tops, tops)]
        weights = [faded(s, top) for s, top in zip(scores, tops)]
        dens = [
            den_ref[place : place + rows] * fade
            + jnp.broadcast_to(jnp.sum(weight, axis=1, keepdims=True), wide)
            for place, fade, weight in zip(places, fades, weights)
        ]
        sums = [
            jnp.dot(weight.astype(bf16), value_ref[...], preferred_element_type=f32)
            for weight in weights
        ]
        for h, place in enumerate(places):
            put(h, (acc_ref[place : place + rows] * fades[h] + sums[h]) / dens[h])

    out = jnp.dot(row_ref[...], weight_ref[...], preferred_element_type=f32).astype(bf16)
    start = 0
    for out_ref in outs:
        out_ref[...] = out[start : start + out_ref.shape[0]]
        start += out_ref.shape[0]


def pair_sum_kernel(keep_ref, got_ref, *outs):
    step = outs[0].shape[0]
    for i, out in enumerate(outs):
        rows = slice(i * step, (i + 1) * step)
        total = keep_ref[rows].astype(f32) + got_ref[rows].astype(f32)
        out[...] = total.astype(out.dtype)


def final_kernel(*refs):
    total = refs[0][...].astype(f32)
    for ref in refs[1:-1]:
        total = total + ref[...].astype(f32)
    refs[-1][...] = total.astype(bf16)


def layer(
    tokens,
    norm_gain,
    w_query,
    w_key,
    w_value,
    w_conv_value,
    w_conv_pre,
    w_conv_post,
    conv_taps,
    log_gate_cache,
    w_out_conv,
    w_out_attn,
):
    n_sp, n_fs, n_tp = lax.axis_size("sp"), lax.axis_size("fs"), lax.axis_size("tp")
    step, width = tokens.shape
    lane_rows = n_fs * step
    block_rows = n_tp * lane_rows
    channels = w_conv_post.shape[1]
    head_dim = w_key.shape[1]
    heads = w_query.shape[1] // head_dim

    def swapped(x):
        return lax.ppermute(x, "tp", [(0, 1), (1, 0)])

    def crossed(x, k):
        return lax.ppermute(x, "fs", [(i, i ^ k) for i in range(n_fs)])

    def raised(x, shift):
        route = [(i, (i + shift) % n_sp) for i in range(n_sp) if i + shift < n_sp or RING[shift]]
        return lax.ppermute(x, "sp", route)

    def call(kernel, out_shape, scratch, mib, *operands, in_specs=None, work=0):
        extra = {} if in_specs is None else {"in_specs": in_specs}
        if work:
            extra["cost_estimate"] = pl.CostEstimate(
                flops=work, transcendentals=0, bytes_accessed=0
            )
        return pl.pallas_call(
            kernel,
            out_shape=out_shape,
            scratch_shapes=scratch,
            compiler_params=kernel_params(mib),
            **extra,
        )(*operands)

    mask = call(mask_kernel, shape_of(block_rows, block_rows, f32), [], 4, work=MASK_WORK)
    normed = call(
        norm_kernel,
        shape_of(step, width),
        [],
        4,
        tokens,
        norm_gain.reshape(1, width),
        work=NORM_WORK,
    )
    w_post, w_pre, w_conv = w_conv_post, w_conv_pre, w_conv_value
    gates, taps = log_gate_cache, conv_taps
    own = [normed] + [crossed(normed, k) for k in range(1, n_fs)]
    other = [swapped(x) for x in own]
    pair = call(
        functools.partial(pair_kernel, n_fs),
        shape_of(lane_rows, 2 * head_dim),
        [pltpu.VMEM((lane_rows, width), bf16)],
        8,
        *own,
        w_key,
        w_value,
        work=SMALL_WORK,
    )
    halves = [pair, swapped(pair)]
    for shift in range(2, n_sp):
        piece = raised(pair, shift)
        halves += [piece, swapped(piece)]
    mixed, rise = call(
        functools.partial(gate_kernel, n_fs),
        (shape_of(block_rows, channels), shape_of(lane_rows + EDGE, 2 * head_dim)),
        [],
        16,
        *own,
        *other,
        w_pre,
        w_conv,
        pair,
        work=SMALL_WORK,
    )
    queries, post = call(
        functools.partial(query_kernel, n_fs),
        (shape_of(block_rows, heads * head_dim), shape_of(block_rows, channels)),
        [],
        16,
        *own,
        *other,
        w_query,
        w_post,
        work=SMALL_WORK,
    )
    near = raised(rise, 1)
    far = swapped(near)
    held_shapes = (shape_of(heads * block_rows, head_dim, f32),) * 3
    *held, column, tap_rows = call(
        early_kernel,
        (
            *held_shapes,
            jax.ShapeDtypeStruct((heads, block_rows, 8), f32),
            shape_of(taps.shape[0], channels, f32),
        ),
        [pltpu.VMEM((block_rows, head_dim), bf16)] * 2 + [pltpu.VMEM((block_rows, 8), f32)],
        16,
        queries,
        gates,
        mask,
        taps,
        *halves[:2],
        work=SMALL_WORK,
    )
    held = call(
        later_kernel,
        held_shapes,
        [pltpu.VMEM(((n_sp - 2) * block_rows, head_dim), bf16)] * 2,
        16,
        queries,
        gates,
        column,
        *held,
        *halves[2:],
        work=SMALL_WORK,
    )
    conv_out = call(
        functools.partial(conv_kernel, n_fs),
        shape_of(block_rows, channels),
        [pltpu.VMEM((block_rows + EDGE, channels), f32), pltpu.VMEM((block_rows, channels), f32)],
        4,
        post,
        mixed,
        near,
        tap_rows,
        work=SMALL_WORK,
    )
    w_out = call(
        stack_kernel,
        shape_of(w_out_conv.shape[0] + w_out_attn.shape[0], width),
        [],
        8,
        w_out_conv,
        w_out_attn,
    )

    def mixed_rows(first):
        return call(
            functools.partial(mixer_kernel, first),
            tuple(shape_of(count * step, width) for count in (1, n_fs - 1)),
            [pltpu.VMEM((block_rows, head_dim), bf16)] * 2
            + [pltpu.VMEM((lane_rows, channels + heads * head_dim), bf16)],
            16,
            queries,
            conv_out,
            gates,
            column,
            *held,
            near,
            far,
            w_out,
            work=SMALL_WORK,
        )

    counts = (1, n_fs - 1)
    sends = mixed_rows(0)
    gots = [swapped(send) for send in sends]
    keeps = mixed_rows(lane_rows)
    parts = list(range(n_fs - 1, -1, -1))
    sums = []
    for count, keep, got in zip(counts, keeps, gots):
        group, parts = parts[:count], parts[count:]
        pieces = call(
            pair_sum_kernel,
            tuple(shape_of(step, width, bf16 if k else f32) for k in group),
            [],
            8,
            keep,
            got,
        )
        sums += [crossed(piece, k) if k else piece for k, piece in zip(group, pieces)]
    return call(final_kernel, shape_of(step, width), [], 4, *sums)


def passed_along(block, axis, distance):
    devices = range(lax.axis_size(axis))
    route = [(i - distance, i) for i in devices if i - distance in devices]
    return lax.ppermute(block, axis, route)


def shards(
    tokens,
    norm_gain,
    w_query,
    w_key,
    w_value,
    w_conv_value,
    w_conv_pre,
    w_conv_post,
    conv_taps,
    log_gate_cache,
    w_out_conv,
    w_out_attn,
):
    float_rows = tokens.astype(jnp.float32)
    scaled = float_rows * lax.rsqrt(
        jnp.mean(float_rows * float_rows, axis=1, keepdims=True) + epsilon
    )
    normed_own = (scaled * norm_gain).astype(jnp.bfloat16)
    normed = lax.all_gather(normed_own, ("fs", "tp"), axis=0, tiled=True)
    block_rows = normed.shape[0]
    channels = w_conv_post.shape[1]
    head_dim = w_key.shape[1]
    local_heads = w_query.shape[1] // head_dim
    group = lax.axis_index(("fs", "tp"))
    local_weight = jnp.concatenate([w_conv_post, w_conv_pre, w_conv_value, w_query], axis=1)
    projected = jnp.dot(normed, local_weight, preferred_element_type=jnp.float32).astype(
        jnp.bfloat16
    )
    post_gate = projected[:, :channels]
    pre_gate = projected[:, channels : 2 * channels]
    conv_value = projected[:, 2 * channels : 3 * channels]
    queries = projected[:, 3 * channels :].reshape(block_rows, local_heads, head_dim)
    mixed_in = (pre_gate.astype(jnp.float32) * conv_value.astype(jnp.float32)).astype(jnp.bfloat16)
    kernel = conv_taps.shape[0]
    carried = passed_along(mixed_in[block_rows - (kernel - 1) :], "sp", 1)
    extended = jnp.concatenate([carried, mixed_in], axis=0).astype(jnp.float32)
    tap_weights = lax.dynamic_slice_in_dim(conv_taps, group * channels, channels, 1).astype(
        jnp.float32
    )
    conv_sum = tap_weights[0] * extended[0:block_rows]
    for offset in range(1, kernel):
        conv_sum = conv_sum + tap_weights[offset] * extended[offset : offset + block_rows]
    conv_out = (post_gate.astype(jnp.float32) * conv_sum).astype(jnp.bfloat16)
    core_index = lax.axis_index("tp")
    half_rows = block_rows // 2
    own_rows = lax.dynamic_slice_in_dim(normed, core_index * half_rows, half_rows, 0)
    pair_weight = jnp.concatenate([w_key, w_value], axis=1)
    pair_rows = jnp.dot(own_rows, pair_weight, preferred_element_type=jnp.float32).astype(
        jnp.bfloat16
    )
    key_half = pair_rows[:, :head_dim]
    value_half = pair_rows[:, head_dim:]
    head_gates = lax.dynamic_slice_in_dim(log_gate_cache, group * local_heads, local_heads, 0)
    anchor = lax.axis_index("sp") * block_rows
    gate_query = lax.dynamic_slice_in_dim(head_gates, anchor, block_rows, 1).T
    sequence_places = anchor + lax.iota(jnp.int32, block_rows)
    score_scale = head_dim ** (-0.5)

    def absorb(carried_state, key_block, value_block, sub_start):
        running_max, running_sum, weighted = carried_state
        sub_width = key_block.shape[0]
        scores = (
            jnp.einsum("qhd,kd->qhk", queries, key_block, preferred_element_type=jnp.float32)
            * score_scale
        )
        gate_keys = lax.dynamic_slice_in_dim(head_gates, sub_start, sub_width, 1)
        scores = scores + gate_query[:, :, None] - gate_keys[None, :, :]
        key_positions = sub_start + lax.iota(jnp.int32, sub_width)
        scores = jnp.where(
            sequence_places[:, None, None] >= key_positions[None, None, :], scores, masked_score
        )
        new_max = jnp.maximum(running_max, jnp.max(scores, axis=2))
        rescale = jnp.exp(running_max - new_max)
        weights = jnp.exp(scores - new_max[:, :, None])
        running_sum = running_sum * rescale + jnp.sum(weights, axis=2)
        weighted = weighted * rescale[:, :, None] + jnp.einsum(
            "qhk,kd->qhd",
            weights.astype(jnp.bfloat16),
            value_block,
            preferred_element_type=jnp.float32,
        )
        return (new_max, running_sum, weighted)

    initial = (
        jnp.full((block_rows, local_heads), masked_score, jnp.float32),
        jnp.zeros((block_rows, local_heads), jnp.float32),
        jnp.zeros((block_rows, local_heads, head_dim), jnp.float32),
    )
    key_piece = lax.all_gather(key_half, ("sp", "tp"), axis=0, tiled=True)
    value_piece = lax.all_gather(value_half, ("sp", "tp"), axis=0, tiled=True)
    key_count = key_piece.shape[0]
    sub_width = 512

    def sweep_keys(current):

        def absorb_step(running, step_index):
            sub_start = step_index * sub_width
            key_block = lax.dynamic_slice_in_dim(key_piece, sub_start, sub_width, 0)
            value_block = lax.dynamic_slice_in_dim(value_piece, sub_start, sub_width, 0)
            return (absorb(running, key_block, value_block, sub_start), None)

        result, _ = lax.scan(
            absorb_step, current, jnp.arange(key_count // sub_width, dtype=jnp.int32)
        )
        return result

    def keep_state(current):
        return current

    _, running_sum, weighted = lax.cond(
        jnp.int32(0) <= anchor + block_rows - 1, sweep_keys, keep_state, initial
    )
    attn_out = (
        (weighted / running_sum[:, :, None])
        .astype(jnp.bfloat16)
        .reshape(block_rows, local_heads * head_dim)
    )
    return lax.psum_scatter(
        (
            jnp.dot(conv_out, w_out_conv, preferred_element_type=jnp.float32)
            + jnp.dot(attn_out, w_out_attn, preferred_element_type=jnp.float32)
        ).astype(jnp.bfloat16),
        ("fs", "tp"),
        scatter_dimension=0,
        tiled=True,
    )


def solution(mesh):
    few = mesh.shape["sp"] == 4
    placed = (
        P(("sp", "fs", "tp"), None),
        P(),
        P(None, ("fs", "tp")),
        P(None, "fs"),
        P(None, "fs"),
        P(None, ("fs", "tp")),
        P(None, ("fs", "tp")),
        P(None, ("fs", "tp")),
        P(),
        P(),
        P(("fs", "tp"), None),
        P(("fs", "tp"), None),
    )
    return jax.shard_map(
        layer if few else shards,
        mesh=mesh,
        in_specs=placed,
        out_specs=P(("sp", "fs", "tp"), None),
        check_vma=False,
    )
```

```python
import functools
import math
import jax
import jax.numpy as jnp
from jax import lax
from jax.experimental import pallas as pl
from jax.experimental.pallas import tpu as pltpu
from jax.sharding import PartitionSpec as P

epsilon = 1e-06
masked_score = -1e30
log2e = math.log2(math.e)
f32 = jnp.float32
bf16 = jnp.bfloat16
EDGE = 16
RING = (False, False, True, True)
NORM_WORK = 20000000000
SMALL_WORK = 2000000000


def kernel_params(mib):
    return pltpu.CompilerParams(vmem_limit_bytes=mib * 1024 * 1024)


def shape_of(rows, cols, dtype=bf16):
    return jax.ShapeDtypeStruct((rows, cols), dtype)


def mask_kernel(out_ref):
    query_place = lax.broadcasted_iota(jnp.int32, out_ref.shape, 0)
    key_place = lax.broadcasted_iota(jnp.int32, out_ref.shape, 1)
    out_ref[...] = jnp.where(query_place >= key_place, 0.0, masked_score)


def normalized(tokens, gain):
    rows = tokens.astype(f32)
    scale = lax.rsqrt(jnp.mean(rows * rows, axis=1, keepdims=True) + epsilon)
    return (rows * scale * gain).astype(bf16)


def pair_kernel(n_fs, *refs):
    chunks, (gain_ref, w_key, w_value, out_ref, normed_ref, rows_ref) = refs[:n_fs], refs[n_fs:]
    step = chunks[0].shape[0]
    f = lax.axis_index("fs")
    for k in range(n_fs):
        rows = normalized(chunks[k][...], gain_ref[...])
        normed_ref[(n_fs - 1 - k) * step : (n_fs - k) * step] = rows
        rows_ref[pl.ds(pl.multiple_of((f ^ k) * step, step), step)] = rows
    weight = jnp.concatenate([w_key[...], w_value[...]], axis=1)
    out_ref[...] = jnp.dot(rows_ref[...], weight, preferred_element_type=f32).astype(bf16)


def place_pairs(pieces, key_ref, value_ref):
    head_dim = key_ref.shape[1]
    t = lax.axis_index("tp")
    n_fs = lax.axis_size("fs")
    step = key_ref.shape[0] // (2 * n_fs * len(pieces))
    for k, (near, far) in enumerate(pieces):
        for lane, piece in ((t, near), (1 - t, far)):
            for g in range(n_fs):
                place = (k * n_fs + g) * 2 * step + lane * step
                place = pl.ds(pl.multiple_of(place, step), step)
                key_ref[place] = piece[g * step : (g + 1) * step, :head_dim]
                value_ref[place] = piece[g * step : (g + 1) * step, head_dim:]


def gate_row(gates_ref, h, heads, origin, block_rows):
    group = lax.axis_index("fs") * lax.axis_size("tp") + lax.axis_index("tp")
    place = pl.multiple_of(jnp.maximum(origin, 0) * block_rows, block_rows)
    return gates_ref[pl.ds(group * heads + h, 1), pl.ds(place, block_rows)] * log2e


def score(queries, keys, gate_q, gate_k, origin):
    scale = queries.shape[1] ** (-0.5) * log2e
    s = lax.dot_general(
        queries, keys, (((1,), (1,)), ((), ())), preferred_element_type=f32
    )
    return s * scale + gate_q - jnp.where(origin >= 0, gate_k, -masked_score)


def faded(s, top):
    return jnp.exp2(s - jnp.concatenate([top] * (s.shape[1] // top.shape[1]), axis=1))


def fold_blocks(q_ref, gates_ref, column_ref, blocks, masks, held, outs):
    acc_ref, top_ref, den_ref = outs
    block_rows = q_ref.shape[0]
    head_dim = acc_ref.shape[1]
    heads = q_ref.shape[1] // head_dim
    tile = block_rows // 2
    tiles = [(h, i) for h in range(heads) for i in range(0, block_rows, tile)]
    places = [slice(h * block_rows + i, h * block_rows + i + tile) for h, i in tiles]
    scores = []
    for h, i in tiles:
        queries = q_ref[i : i + tile, h * head_dim : (h + 1) * head_dim]
        gate_q = column_ref[h, i : i + tile, 0:1]
        row = []
        for keys, values, origin in blocks:
            gate_k = gate_row(gates_ref, h, heads, origin, block_rows)
            s = score(queries, keys, gate_q, gate_k, origin)
            row.append(s + masks[i // tile] if masks else s)
        scores.append(row)
    wide = (tile, head_dim)
    tops = [
        jnp.broadcast_to(
            jnp.max(functools.reduce(jnp.maximum, row), axis=1, keepdims=True), wide
        )
        for row in scores
    ]
    if held:
        held_tops = [held[1][place] for place in places]
        tops = [jnp.maximum(top, held_top) for top, held_top in zip(tops, held_tops)]
        fades = [jnp.exp2(held_top - top) for top, held_top in zip(tops, held_tops)]
    weights = [[faded(s, top) for s in row] for row, top in zip(scores, tops)]
    dens = [
        jnp.broadcast_to(jnp.sum(sum(row), axis=1, keepdims=True), wide) for row in weights
    ]
    for n, place in enumerate(places):
        total = sum(
            jnp.dot(weight.astype(bf16), values, preferred_element_type=f32)
            for weight, (keys, values, origin) in zip(weights[n], blocks)
        )
        den = dens[n]
        if held:
            total = total + held[0][place] * fades[n]
            den = den + held[2][place] * fades[n]
        acc_ref[place] = total
        top_ref[place] = tops[n]
        den_ref[place] = den


def early_kernel(*refs):
    q_ref, gates_ref, mask_ref, taps_ref, near_ref, far_ref = refs[:6]
    outs, (column_ref, tap_ref, key_ref, value_ref, natural_ref) = refs[6:9], refs[9:]
    group = lax.axis_index("fs") * lax.axis_size("tp") + lax.axis_index("tp")
    channels = tap_ref.shape[1]
    lanes = pl.ds(pl.multiple_of(group * channels, channels), channels)
    tap_ref[...] = taps_ref[:, lanes].astype(f32)
    place_pairs(((near_ref, far_ref),), key_ref, value_ref)
    z = lax.axis_index("sp")
    block_rows = q_ref.shape[0]
    heads = column_ref.shape[0]
    n_fs = lax.axis_size("fs")
    step = block_rows // (2 * n_fs)
    places = row_places(n_fs, step)
    for h in range(heads):
        row = gate_row(gates_ref, h, heads, z, block_rows)
        natural_ref[...] = jnp.broadcast_to(row, (8, block_rows)).T
        for i, place in enumerate(places):
            column_ref[h, i * step : (i + 1) * step] = natural_ref[pl.ds(place, step)]
    masks = []
    for i in range(0, 2 * n_fs, n_fs):
        piece = [mask_ref[pl.ds(place, step)] for place in places[i : i + n_fs]]
        masks.append(jnp.concatenate(piece, axis=0))
    blocks = [(key_ref[...], value_ref[...], z)]
    fold_blocks(q_ref, gates_ref, column_ref, blocks, masks, None, outs)


def later_kernel(*refs):
    q_ref, gates_ref, column_ref = refs[:3]
    held, outs, (key_ref, value_ref) = refs[3:6], refs[-5:-2], refs[-2:]
    pieces = tuple(zip(refs[6:-5:2], refs[7:-5:2]))
    z = lax.axis_index("sp")
    block_rows = q_ref.shape[0]

    def keep():
        for source, out in zip(held, outs):
            out[...] = source[...]

    def fold(count):
        rows = slice(0, count * block_rows)
        place_pairs(pieces[:count], key_ref.at[rows], value_ref.at[rows])
        blocks = []
        for k in range(count):
            rows = slice(k * block_rows, (k + 1) * block_rows)
            blocks.append((key_ref[rows], value_ref[rows], z - 2 - k))
        fold_blocks(q_ref, gates_ref, column_ref, blocks, None, held, outs)

    pl.when(z < 2)(keep)
    for count in range(1, len(pieces) + 1):
        pl.when(z - 1 == count)(functools.partial(fold, count))


def row_places(n_fs, step):
    f = lax.axis_index("fs")
    t = lax.axis_index("tp")
    return [
        pl.multiple_of((f ^ k) * 2 * step + lane * step, step)
        for lane in (1 - t, t)
        for k in range(n_fs - 1, -1, -1)
    ]


def gate_kernel(n_fs, *refs):
    other, (near_ref, gain_ref, w_pre, w_conv, pair_ref) = refs[:n_fs], refs[n_fs : n_fs + 5]
    mixed_ref, rise_ref, rows_ref = refs[n_fs + 5 :]
    step = other[0].shape[0]
    for i, ref in enumerate(other[::-1]):
        rows_ref[i * step : (i + 1) * step] = normalized(ref[...], gain_ref[...])
    rows_ref[n_fs * step :] = near_ref[...]
    rows = rows_ref[...]
    weight = jnp.concatenate([w_pre[...], w_conv[...]], axis=1)
    gated = jnp.dot(rows, weight, preferred_element_type=f32).astype(bf16).astype(f32)
    channels = w_pre.shape[1]
    mixed = (gated[:, :channels] * gated[:, channels:]).astype(bf16)
    for i, place in enumerate(row_places(n_fs, step)):
        mixed_ref[pl.ds(place, step)] = mixed[i * step : (i + 1) * step]
    lane_rows = pair_ref.shape[0]
    rise_ref[:lane_rows] = pair_ref[...]
    last = mixed_ref[mixed_ref.shape[0] - EDGE :]
    rise_ref[lane_rows:] = jnp.concatenate([last] * (rise_ref.shape[1] // channels), axis=1)


def query_kernel(rows_ref, w_query, w_post, q_ref, post_ref):
    rows = rows_ref[...]
    q_ref[...] = jnp.dot(rows, w_query[...], preferred_element_type=f32).astype(bf16)
    post_ref[...] = jnp.dot(rows, w_post[...], preferred_element_type=f32).astype(bf16)


def stack_kernel(top_ref, low_ref, out_ref):
    out_ref[: top_ref.shape[0]] = top_ref[...]
    out_ref[top_ref.shape[0] :] = low_ref[...]


def conv_kernel(n_fs, post_ref, mixed_ref, risen_ref, taps_ref, out_ref, extended_ref, sum_ref):
    block_rows, channels = mixed_ref.shape
    taps = taps_ref.shape[0]
    halo = risen_ref[risen_ref.shape[0] - EDGE :, :channels].astype(f32)
    extended_ref[0:EDGE] = jnp.where(lax.axis_index("sp") > 0, halo, 0.0)
    extended_ref[EDGE:] = mixed_ref[...].astype(f32)
    tap_rows = taps_ref[...]
    first = EDGE - (taps - 1)
    conv_sum = tap_rows[0:1] * extended_ref[first : first + block_rows]
    for i in range(1, taps):
        conv_sum = conv_sum + tap_rows[i : i + 1] * extended_ref[first + i : first + i + block_rows]
    sum_ref[...] = conv_sum
    step = block_rows // (2 * n_fs)
    for i, place in enumerate(row_places(n_fs, step)):
        rows = slice(i * step, (i + 1) * step)
        out_ref[rows] = (post_ref[rows].astype(f32) * sum_ref[pl.ds(place, step)]).astype(bf16)


def mixer_kernel(first, *refs):
    q_ref, conv_ref, gates_ref, column_ref, acc_ref, top_ref, den_ref = refs[:7]
    near_ref, far_ref, weight_ref = refs[7:10]
    outs, (key_ref, value_ref, row_ref) = refs[10:-3], refs[-3:]
    block_rows = q_ref.shape[0]
    head_dim = key_ref.shape[1]
    channels = conv_ref.shape[1]
    heads = q_ref.shape[1] // head_dim
    rows = sum(out_ref.shape[0] for out_ref in outs)
    origin = lax.axis_index("sp") - 1
    row_ref[:, :channels] = conv_ref[first : first + rows]

    def put(h, value):
        place = channels + h * head_dim
        row_ref[:, place : place + head_dim] = value.astype(bf16)

    @pl.when(origin < 0)
    def alone():
        for h in range(heads):
            place = h * block_rows + first
            put(h, acc_ref[place : place + rows] / den_ref[place : place + rows])

    @pl.when(origin >= 0)
    def joined():
        place_pairs(((near_ref, far_ref),), key_ref, value_ref)
        places = [h * block_rows + first for h in range(heads)]
        scores = []
        for h in range(heads):
            queries = q_ref[first : first + rows, h * head_dim : (h + 1) * head_dim]
            gate_q = column_ref[h, first : first + rows, 0:1]
            gate_k = gate_row(gates_ref, h, heads, origin, block_rows)
            scores.append(score(queries, key_ref[...], gate_q, gate_k, origin))
        wide = (rows, head_dim)
        held_tops = [top_ref[place : place + rows] for place in places]
        tops = [
            jnp.maximum(top, jnp.broadcast_to(jnp.max(s, axis=1, keepdims=True), wide))
            for top, s in zip(held_tops, scores)
        ]
        fades = [jnp.exp2(held_top - top) for held_top, top in zip(held_tops, tops)]
        weights = [faded(s, top) for s, top in zip(scores, tops)]
        dens = [
            den_ref[place : place + rows] * fade
            + jnp.broadcast_to(jnp.sum(weight, axis=1, keepdims=True), wide)
            for place, fade, weight in zip(places, fades, weights)
        ]
        sums = [
            jnp.dot(weight.astype(bf16), value_ref[...], preferred_element_type=f32)
            for weight in weights
        ]
        for h, place in enumerate(places):
            put(h, (acc_ref[place : place + rows] * fades[h] + sums[h]) / dens[h])

    out = jnp.dot(row_ref[...], weight_ref[...], preferred_element_type=f32).astype(bf16)
    start = 0
    for out_ref in outs:
        out_ref[...] = out[start : start + out_ref.shape[0]]
        start += out_ref.shape[0]


def pair_sum_kernel(keep_ref, got_ref, *outs):
    step = outs[0].shape[0]
    for i, out in enumerate(outs):
        rows = slice(i * step, (i + 1) * step)
        total = keep_ref[rows].astype(f32) + got_ref[rows].astype(f32)
        out[...] = total.astype(out.dtype)


def final_kernel(*refs):
    total = refs[0][...].astype(f32)
    for ref in refs[1:-1]:
        total = total + ref[...].astype(f32)
    refs[-1][...] = total.astype(bf16)


def layer(
    tokens,
    norm_gain,
    w_query,
    w_key,
    w_value,
    w_conv_value,
    w_conv_pre,
    w_conv_post,
    conv_taps,
    log_gate_cache,
    w_out_conv,
    w_out_attn,
):
    n_sp, n_fs, n_tp = lax.axis_size("sp"), lax.axis_size("fs"), lax.axis_size("tp")
    step, width = tokens.shape
    lane_rows = n_fs * step
    block_rows = n_tp * lane_rows
    channels = w_conv_post.shape[1]
    head_dim = w_key.shape[1]
    heads = w_query.shape[1] // head_dim

    def swapped(x):
        return lax.ppermute(x, "tp", [(0, 1), (1, 0)])

    def crossed(x, k):
        return lax.ppermute(x, "fs", [(i, i ^ k) for i in range(n_fs)])

    def raised(x, shift):
        route = [(i, (i + shift) % n_sp) for i in range(n_sp) if i + shift < n_sp or RING[shift]]
        return lax.ppermute(x, "sp", route)

    def call(kernel, out_shape, scratch, mib, *operands, in_specs=None, work=0):
        extra = {} if in_specs is None else {"in_specs": in_specs}
        if work:
            extra["cost_estimate"] = pl.CostEstimate(
                flops=work, transcendentals=0, bytes_accessed=0
            )
        return pl.pallas_call(
            kernel,
            out_shape=out_shape,
            scratch_shapes=scratch,
            compiler_params=kernel_params(mib),
            **extra,
        )(*operands)

    mask = call(mask_kernel, shape_of(block_rows, block_rows, f32), [], 4, work=NORM_WORK)
    gain = norm_gain.reshape(1, width)
    w_post, w_pre, w_conv = w_conv_post, w_conv_pre, w_conv_value
    gates, taps = log_gate_cache, conv_taps
    own = [tokens] + [crossed(tokens, k) for k in range(1, n_fs)]
    other = [swapped(x) for x in own]
    pair, near_rows = call(
        functools.partial(pair_kernel, n_fs),
        (shape_of(lane_rows, 2 * head_dim), shape_of(lane_rows, width)),
        [pltpu.VMEM((lane_rows, width), bf16)],
        8,
        *own,
        gain,
        w_key,
        w_value,
        work=SMALL_WORK,
    )
    halves = [pair, swapped(pair)]
    for shift in range(2, n_sp):
        piece = raised(pair, shift)
        halves += [piece, swapped(piece)]
    mixed, rise, rows = call(
        functools.partial(gate_kernel, n_fs),
        (
            shape_of(block_rows, channels),
            shape_of(lane_rows + EDGE, 2 * head_dim),
            shape_of(block_rows, width),
        ),
        [],
        16,
        *other,
        near_rows,
        gain,
        w_pre,
        w_conv,
        pair,
        work=SMALL_WORK,
    )
    queries, post = call(
        query_kernel,
        (shape_of(block_rows, heads * head_dim), shape_of(block_rows, channels)),
        [],
        16,
        rows,
        w_query,
        w_post,
        work=SMALL_WORK,
    )
    near = raised(rise, 1)
    far = swapped(near)
    held_shapes = (shape_of(heads * block_rows, head_dim, f32),) * 3
    *held, column, tap_rows = call(
        early_kernel,
        (
            *held_shapes,
            jax.ShapeDtypeStruct((heads, block_rows, 8), f32),
            shape_of(taps.shape[0], channels, f32),
        ),
        [pltpu.VMEM((block_rows, head_dim), bf16)] * 2 + [pltpu.VMEM((block_rows, 8), f32)],
        16,
        queries,
        gates,
        mask,
        taps,
        *halves[:2],
        work=SMALL_WORK,
    )
    held = call(
        later_kernel,
        held_shapes,
        [pltpu.VMEM(((n_sp - 2) * block_rows, head_dim), bf16)] * 2,
        16,
        queries,
        gates,
        column,
        *held,
        *halves[2:],
        work=SMALL_WORK,
    )
    conv_out = call(
        functools.partial(conv_kernel, n_fs),
        shape_of(block_rows, channels),
        [pltpu.VMEM((block_rows + EDGE, channels), f32), pltpu.VMEM((block_rows, channels), f32)],
        4,
        post,
        mixed,
        near,
        tap_rows,
        work=SMALL_WORK,
    )
    w_out = call(
        stack_kernel,
        shape_of(w_out_conv.shape[0] + w_out_attn.shape[0], width),
        [],
        8,
        w_out_conv,
        w_out_attn,
    )

    def mixed_rows(first):
        return call(
            functools.partial(mixer_kernel, first),
            tuple(shape_of(count * step, width) for count in (1, n_fs - 1)),
            [pltpu.VMEM((block_rows, head_dim), bf16)] * 2
            + [pltpu.VMEM((lane_rows, channels + heads * head_dim), bf16)],
            16,
            queries,
            conv_out,
            gates,
            column,
            *held,
            near,
            far,
            w_out,
            work=SMALL_WORK,
        )

    counts = (1, n_fs - 1)
    sends = mixed_rows(0)
    gots = [swapped(send) for send in sends]
    keeps = mixed_rows(lane_rows)
    parts = list(range(n_fs - 1, -1, -1))
    sums = []
    for count, keep, got in zip(counts, keeps, gots):
        group, parts = parts[:count], parts[count:]
        pieces = call(
            pair_sum_kernel,
            tuple(shape_of(step, width, bf16 if k else f32) for k in group),
            [],
            8,
            keep,
            got,
        )
        sums += [crossed(piece, k) if k else piece for k, piece in zip(group, pieces)]
    return call(final_kernel, shape_of(step, width), [], 4, *sums)


def passed_along(block, axis, distance):
    devices = range(lax.axis_size(axis))
    route = [(i - distance, i) for i in devices if i - distance in devices]
    return lax.ppermute(block, axis, route)


def shards(
    tokens,
    norm_gain,
    w_query,
    w_key,
    w_value,
    w_conv_value,
    w_conv_pre,
    w_conv_post,
    conv_taps,
    log_gate_cache,
    w_out_conv,
    w_out_attn,
):
    float_rows = tokens.astype(jnp.float32)
    scaled = float_rows * lax.rsqrt(
        jnp.mean(float_rows * float_rows, axis=1, keepdims=True) + epsilon
    )
    normed_own = (scaled * norm_gain).astype(jnp.bfloat16)
    normed = lax.all_gather(normed_own, ("fs", "tp"), axis=0, tiled=True)
    block_rows = normed.shape[0]
    channels = w_conv_post.shape[1]
    head_dim = w_key.shape[1]
    local_heads = w_query.shape[1] // head_dim
    group = lax.axis_index(("fs", "tp"))
    local_weight = jnp.concatenate([w_conv_post, w_conv_pre, w_conv_value, w_query], axis=1)
    projected = jnp.dot(normed, local_weight, preferred_element_type=jnp.float32).astype(
        jnp.bfloat16
    )
    post_gate = projected[:, :channels]
    pre_gate = projected[:, channels : 2 * channels]
    conv_value = projected[:, 2 * channels : 3 * channels]
    queries = projected[:, 3 * channels :].reshape(block_rows, local_heads, head_dim)
    mixed_in = (pre_gate.astype(jnp.float32) * conv_value.astype(jnp.float32)).astype(jnp.bfloat16)
    kernel = conv_taps.shape[0]
    carried = passed_along(mixed_in[block_rows - (kernel - 1) :], "sp", 1)
    extended = jnp.concatenate([carried, mixed_in], axis=0).astype(jnp.float32)
    tap_weights = lax.dynamic_slice_in_dim(conv_taps, group * channels, channels, 1).astype(
        jnp.float32
    )
    conv_sum = tap_weights[0] * extended[0:block_rows]
    for offset in range(1, kernel):
        conv_sum = conv_sum + tap_weights[offset] * extended[offset : offset + block_rows]
    conv_out = (post_gate.astype(jnp.float32) * conv_sum).astype(jnp.bfloat16)
    core_index = lax.axis_index("tp")
    half_rows = block_rows // 2
    own_rows = lax.dynamic_slice_in_dim(normed, core_index * half_rows, half_rows, 0)
    pair_weight = jnp.concatenate([w_key, w_value], axis=1)
    pair_rows = jnp.dot(own_rows, pair_weight, preferred_element_type=jnp.float32).astype(
        jnp.bfloat16
    )
    key_half = pair_rows[:, :head_dim]
    value_half = pair_rows[:, head_dim:]
    head_gates = lax.dynamic_slice_in_dim(log_gate_cache, group * local_heads, local_heads, 0)
    anchor = lax.axis_index("sp") * block_rows
    gate_query = lax.dynamic_slice_in_dim(head_gates, anchor, block_rows, 1).T
    sequence_places = anchor + lax.iota(jnp.int32, block_rows)
    score_scale = head_dim ** (-0.5)

    def absorb(carried_state, key_block, value_block, sub_start):
        running_max, running_sum, weighted = carried_state
        sub_width = key_block.shape[0]
        scores = (
            jnp.einsum("qhd,kd->qhk", queries, key_block, preferred_element_type=jnp.float32)
            * score_scale
        )
        gate_keys = lax.dynamic_slice_in_dim(head_gates, sub_start, sub_width, 1)
        scores = scores + gate_query[:, :, None] - gate_keys[None, :, :]
        key_positions = sub_start + lax.iota(jnp.int32, sub_width)
        scores = jnp.where(
            sequence_places[:, None, None] >= key_positions[None, None, :], scores, masked_score
        )
        new_max = jnp.maximum(running_max, jnp.max(scores, axis=2))
        rescale = jnp.exp(running_max - new_max)
        weights = jnp.exp(scores - new_max[:, :, None])
        running_sum = running_sum * rescale + jnp.sum(weights, axis=2)
        weighted = weighted * rescale[:, :, None] + jnp.einsum(
            "qhk,kd->qhd",
            weights.astype(jnp.bfloat16),
            value_block,
            preferred_element_type=jnp.float32,
        )
        return (new_max, running_sum, weighted)

    initial = (
        jnp.full((block_rows, local_heads), masked_score, jnp.float32),
        jnp.zeros((block_rows, local_heads), jnp.float32),
        jnp.zeros((block_rows, local_heads, head_dim), jnp.float32),
    )
    key_piece = lax.all_gather(key_half, ("sp", "tp"), axis=0, tiled=True)
    value_piece = lax.all_gather(value_half, ("sp", "tp"), axis=0, tiled=True)
    key_count = key_piece.shape[0]
    sub_width = 512

    def sweep_keys(current):

        def absorb_step(running, step_index):
            sub_start = step_index * sub_width
            key_block = lax.dynamic_slice_in_dim(key_piece, sub_start, sub_width, 0)
            value_block = lax.dynamic_slice_in_dim(value_piece, sub_start, sub_width, 0)
            return (absorb(running, key_block, value_block, sub_start), None)

        result, _ = lax.scan(
            absorb_step, current, jnp.arange(key_count // sub_width, dtype=jnp.int32)
        )
        return result

    def keep_state(current):
        return current

    _, running_sum, weighted = lax.cond(
        jnp.int32(0) <= anchor + block_rows - 1, sweep_keys, keep_state, initial
    )
    attn_out = (
        (weighted / running_sum[:, :, None])
        .astype(jnp.bfloat16)
        .reshape(block_rows, local_heads * head_dim)
    )
    return lax.psum_scatter(
        (
            jnp.dot(conv_out, w_out_conv, preferred_element_type=jnp.float32)
            + jnp.dot(attn_out, w_out_attn, preferred_element_type=jnp.float32)
        ).astype(jnp.bfloat16),
        ("fs", "tp"),
        scatter_dimension=0,
        tiled=True,
    )


def solution(mesh):
    few = mesh.shape["sp"] == 4
    placed = (
        P(("sp", "fs", "tp"), None),
        P(),
        P(None, ("fs", "tp")),
        P(None, "fs"),
        P(None, "fs"),
        P(None, ("fs", "tp")),
        P(None, ("fs", "tp")),
        P(None, ("fs", "tp")),
        P(),
        P(),
        P(("fs", "tp"), None),
        P(("fs", "tp"), None),
    )
    return jax.shard_map(
        layer if few else shards,
        mesh=mesh,
        in_specs=placed,
        out_specs=P(("sp", "fs", "tp"), None),
        check_vma=False,
    )
```
